128 devices in a mesh: ep: 16 (over z, x), tp: 8 (over y, core).
Axes of the slice: x: 4, y: 4, z: 4, core: 2. Of those that a mesh axis runs over, the one named last changes fastest.
Arguments:
- mixer_input: bfloat16 [16384, 2048], P(('ep', 'tp')), may hold values from -6 to 6
- log_decay: float32 [16384, 8], P('ep', 'tp'), may hold values from -0.8 to 0
- mixer_gain: float32 [2048], replicated, may hold values from 0.1 to 1.9
- query_weight: bfloat16 [2048, 1024], P(None, 'tp'), may hold values from -0.125 to 0.125
- key_weight: bfloat16 [2048, 1024], P(None, 'tp'), may hold values from -0.125 to 0.125
- value_weight: bfloat16 [2048, 2048], P(None, 'tp'), may hold values from -0.125 to 0.125
- gate_weight: bfloat16 [2048, 2048], P(None, 'tp'), may hold values from -0.125 to 0.125
- head_gain: float32 [2048], P('tp'), may hold values from 0.1 to 1.9
- output_weight: bfloat16 [2048, 2048], P('tp'), may hold values from -0.125 to 0.125
- expert_input: bfloat16 [16384, 2048], P(('ep', 'tp')), may hold values from -6 to 6
- expert_gain: float32 [2048], replicated, may hold values from 0.1 to 1.9
- routes: int32 [16384, 2], P(('ep', 'tp')), may hold values from 0 to 127, as said below
- group_weight: float32 [16384], P(('ep', 'tp')), may hold values from 0.3 to 1
- pair_weight: float32 [16384, 2], P(('ep', 'tp')), may hold values from 0.2 to 1
- expert_gate: bfloat16 [128, 2048, 1024], P(('ep', 'tp')), may hold values from -0.125 to 0.125
- expert_up: bfloat16 [128, 2048, 1024], P(('ep', 'tp')), may hold values from -0.125 to 0.125
- expert_down: bfloat16 [128, 1024, 2048], P(('ep', 'tp')), may hold values from -0.1875 to 0.1875
Outputs:
- mixer_output: bfloat16 [16384, 2048], P(('ep', 'tp'))
- expert_output: bfloat16 [16384, 2048], P(('ep', 'tp'))
The draws below stay inside these ranges and needn't reach their ends.
Inputs may be any that keep to these rules, and one draw needn't show every extreme that they name: `routes`: in the rows of one device each expert is named at most 3 times; one expert is named exactly 3 times in the rows of every device. A row names two different experts of the same group, a group being 32 consecutive expert numbers.
All inputs are finite; a program needn't handle non-finite values.
Results may differ from the reference program's by a relative error of at most 0.023.
Values may be sent and summed in bfloat16 or wider, within the bound.
A program may use at most 128 MiB of HBM per device.

```python
import jax
import jax.numpy as jnp
from jax import lax

D = 2048
RETENTION_HEADS = 8
KEY_DIM = 128
VALUE_DIM = 256
SPAN = 512
FF = 1024
GROUPS = 4
TOPK = 2
TOK_B = 128
KEY_WIDTH = 1024
VALUE_WIDTH = 2048
SEG_ROWS = 1024
FIRST_POSITIONS = 16384
TOKENS_B = 16384
EXPERTS = 128
GROUP_SIZE = 32
CAP = 3
N_EP = 16
N_TP = 8


def draw_log_decay(key, part):
    split_random_keys = jax.random.split(jax.random.fold_in(key, 3), 7)
    fast_share = 0.5
    fast_heads = jax.random.uniform(split_random_keys[0], (RETENTION_HEADS,)) < fast_share
    fast_rate = 1.0 / jax.random.uniform(split_random_keys[1], (RETENTION_HEADS,), minval=30.0, maxval=100.0)
    slow_rate = jax.random.uniform(split_random_keys[2], (RETENTION_HEADS,), minval=0.1, maxval=0.5) / FIRST_POSITIONS
    head_rate = jnp.where(fast_heads, fast_rate, slow_rate)
    segments = FIRST_POSITIONS // SEG_ROWS
    segment_scale = jnp.exp(jax.random.uniform(split_random_keys[3], (segments,), minval=-0.7, maxval=0.7))
    row_scale = jnp.repeat(segment_scale, SEG_ROWS)
    jitter = jax.random.uniform(split_random_keys[4], (FIRST_POSITIONS, RETENTION_HEADS), minval=0.5, maxval=1.5)
    decay_factor = -head_rate[None, :] * row_scale[:, None] * jitter
    spike_rows = jax.random.randint(split_random_keys[5], (2,), 0, FIRST_POSITIONS)
    spike_loss = jnp.log(jax.random.uniform(split_random_keys[6], (2, RETENTION_HEADS), minval=0.5, maxval=0.8))
    position_list = jnp.arange(FIRST_POSITIONS)
    for index_value in range(2):
        decay_factor = decay_factor + jnp.where(position_list[:, None] == spike_rows[index_value], spike_loss[index_value][None, :], 0.0)
    return decay_factor.astype(jnp.float32)


def draw_routes(key, part):
    base_key = jax.random.fold_in(key, 7)
    chosen_key, block_base = jax.random.split(base_key)
    full_expert = jax.random.randint(chosen_key, (), 0, EXPERTS)
    pair_count = EXPERTS // 2

    def one_block(block_key):
        split_random_keys = jax.random.split(block_key, GROUPS + 3)
        orders = jnp.stack([jax.random.permutation(split_random_keys[group], GROUP_SIZE) for group in range(GROUPS)])
        labels = (orders + GROUP_SIZE * jnp.arange(GROUPS)[:, None]).reshape(-1).astype(jnp.int32)
        location = jnp.argmax(labels == full_expert)
        full_pair = location // 2
        slot_pairs = jnp.repeat(jnp.arange(pair_count), CAP)
        rank_order = jax.random.permutation(split_random_keys[GROUPS], pair_count * CAP)
        scores = jnp.where(slot_pairs == full_pair, rank_order, rank_order + pair_count * CAP)
        picked = jnp.argsort(scores)[:TOK_B]
        token_pairs = slot_pairs[picked][jax.random.permutation(split_random_keys[GROUPS + 1], TOK_B)]
        swapped = jax.random.randint(split_random_keys[GROUPS + 2], (TOK_B,), 0, 2)
        first_id = labels[2 * token_pairs + swapped]
        second = labels[2 * token_pairs + 1 - swapped]
        return jnp.stack([first_id, second], axis=1)
    block_keys = jax.random.split(block_base, TOKENS_B // TOK_B)
    return jax.vmap(one_block)(block_keys).reshape(TOKENS_B, TOPK).astype(jnp.int32)


def block_levels(key, extent, cuts, smallest, top_value):
    def one(dim, parts):
        draws = jax.random.uniform(jax.random.fold_in(jax.random.fold_in(key, 6), dim), (parts,), jnp.float32, smallest / len(cuts), top_value / len(cuts))
        return jnp.repeat(jnp.exp(draws), extent[dim] // parts).reshape((-1,) + (1,) * (len(extent) - dim - 1))

    loudness = one(*cuts[0])
    for cut in cuts[1:]:
        loudness = loudness * one(*cut)
    return loudness


def noise(key, shape, scale, reach, cuts=(), held_as=jnp.bfloat16):
    entries = jax.random.normal(key, shape, jnp.float32) * scale
    if len(cuts) > 0:
        entries = block_levels(key, shape, cuts, -0.22, 0.18) * entries
    return jnp.clip(entries, min=-reach, max=reach).astype(held_as)


def setup_inputs(seed: int = 0) -> dict:
    arg_keys = jax.random.split(jax.random.key(seed), 18)
    mixer_input = noise(arg_keys[0], (FIRST_POSITIONS, D), 1.0, 6.0, ((0, 128),))
    log_decay = draw_log_decay(jax.random.fold_in(arg_keys[17], 71), 0)
    mixer_gain = jnp.clip(1.0 + 0.18 * jax.random.normal(arg_keys[2], (D,), jnp.float32), 0.1, 1.9)
    query_weight = noise(arg_keys[3], (D, KEY_WIDTH), D ** -0.5, 0.125, ((1, 8),))
    key_weight = noise(arg_keys[4], (D, KEY_WIDTH), D ** -0.5, 0.125, ((1, 8),))
    value_weight = noise(arg_keys[5], (D, VALUE_WIDTH), D ** -0.5, 0.125, ((1, 8),))
    gate_weight = noise(arg_keys[6], (D, VALUE_WIDTH), D ** -0.5, 0.125, ((1, 8),))
    head_gain = jnp.clip(1.0 + 0.18 * jax.random.normal(arg_keys[7], (VALUE_WIDTH,), jnp.float32), 0.1, 1.9)
    output_weight = noise(arg_keys[8], (VALUE_WIDTH, D), VALUE_WIDTH ** -0.5, 0.125, ((0, 8),))
    expert_input = noise(arg_keys[9], (TOKENS_B, D), 1.0, 6.0, ((0, 128),))
    expert_gain = jnp.clip(1.0 + 0.18 * jax.random.normal(arg_keys[10], (D,), jnp.float32), 0.1, 1.9)
    routes = draw_routes(jax.random.fold_in(arg_keys[17], 71), 0)
    group_weight = jnp.clip(0.3 + 0.7 * jax.random.uniform(arg_keys[12], (TOKENS_B,), jnp.float32) ** block_levels(arg_keys[12], (TOKENS_B,), ((0, 128),), -0.2, 0.2), 0.3, 1.0)
    pair_weight = jnp.clip(0.2 + 0.8 * jax.random.uniform(arg_keys[13], (TOKENS_B, TOPK), jnp.float32) ** block_levels(arg_keys[13], (TOKENS_B, TOPK), ((0, 128),), -0.2, 0.2), 0.2, 1.0)
    expert_gate = noise(arg_keys[14], (EXPERTS, D, FF), D ** -0.5, 0.125, ((0, 128),))
    expert_up = noise(arg_keys[15], (EXPERTS, D, FF), D ** -0.5, 0.125, ((0, 128),))
    expert_down = noise(arg_keys[16], (EXPERTS, FF, D), FF ** -0.5, 0.1875, ((0, 128),))
    return dict(mixer_input=mixer_input, log_decay=log_decay, mixer_gain=mixer_gain, query_weight=query_weight, key_weight=key_weight, value_weight=value_weight, gate_weight=gate_weight, head_gain=head_gain, output_weight=output_weight, expert_input=expert_input, expert_gain=expert_gain, routes=routes, group_weight=group_weight, pair_weight=pair_weight, expert_gate=expert_gate, expert_up=expert_up, expert_down=expert_down)


EPSILON = 1e-05
THETA = 10000.0

def layer_norm(matrix, norm_gain):
    matrix = matrix.astype(jnp.float32)
    average = lax.optimization_barrier(jnp.mean(matrix, axis=-1, keepdims=True))
    centred = matrix - average
    spread = lax.optimization_barrier(jnp.mean(centred * centred, axis=-1, keepdims=True))
    return centred * lax.rsqrt(spread + EPSILON) * norm_gain.astype(jnp.float32)

def rotate(values, position):
    halfway = values.shape[-1] // 2
    frequency = THETA ** (-jnp.arange(halfway, dtype=jnp.float32) / halfway)
    angles = position[:, None] * frequency[None, :]
    cosine = jnp.cos(angles)[:, None, :]
    sine_part = jnp.sin(angles)[:, None, :]
    leading = values[..., :halfway]
    trailing = values[..., halfway:]
    return jnp.concatenate([leading * cosine - trailing * sine_part, trailing * cosine + leading * sine_part], axis=-1)

def block_step(state, inputs):
    query_rows, key_rows, value_rows, decay_factor = inputs
    span_len = query_rows.shape[0]
    cumulative = jnp.cumsum(decay_factor, axis=0)
    causal = jnp.arange(span_len)[:, None] >= jnp.arange(span_len)[None, :]
    log_gaps = cumulative.T[:, :, None] - cumulative.T[:, None, :]
    weight = jnp.where(causal[None], jnp.exp(jnp.minimum(log_gaps, 0.0)), 0.0)
    query_float = query_rows.astype(jnp.float32)
    key_float = key_rows.astype(jnp.float32)
    value_float = value_rows.astype(jnp.float32)
    scores = jnp.einsum('thd,shd->hts', query_float, key_float, precision=lax.Precision.HIGHEST)
    decayed = (scores * weight).astype(jnp.bfloat16).astype(jnp.float32)
    within = jnp.einsum('hts,she->the', decayed, value_float, precision=lax.Precision.HIGHEST)
    scaled = query_float * jnp.exp(cumulative)[:, :, None]
    carried = jnp.einsum('thd,hde->the', scaled, state, precision=lax.Precision.HIGHEST)
    span_total = cumulative[-1]
    remain = jnp.exp(span_total[None, :] - cumulative)
    update = jnp.einsum('shd,she->hde', key_float * remain[:, :, None], value_float, precision=lax.Precision.HIGHEST)
    return (state * jnp.exp(span_total)[:, None, None] + update, within + carried)

def token_mixer(mixer_input, log_decay, mixer_gain, query_weight, key_weight, value_weight, gate_weight, head_gain, output_weight):
    normed = layer_norm(mixer_input, mixer_gain).astype(jnp.bfloat16)

    def project(weight):
        return jnp.dot(normed, weight, preferred_element_type=jnp.float32).astype(jnp.bfloat16)
    query = project(query_weight).reshape(FIRST_POSITIONS, RETENTION_HEADS, KEY_DIM)
    keys_all = project(key_weight).reshape(FIRST_POSITIONS, RETENTION_HEADS, KEY_DIM)
    value = project(value_weight).reshape(FIRST_POSITIONS, RETENTION_HEADS, VALUE_DIM)
    gate = project(gate_weight).astype(jnp.float32)
    position = jnp.arange(FIRST_POSITIONS).astype(jnp.float32)
    rot_query = rotate(query.astype(jnp.float32), position).astype(jnp.bfloat16)
    rot_key = rotate(keys_all.astype(jnp.float32), position).astype(jnp.bfloat16)
    blocks = FIRST_POSITIONS // SPAN

    def split_blocks(tensor):
        return tensor.reshape((blocks, SPAN) + tensor.shape[1:])
    state_zero = jnp.zeros((RETENTION_HEADS, KEY_DIM, VALUE_DIM), jnp.float32)
    _, retained = lax.scan(block_step, state_zero, (split_blocks(rot_query), split_blocks(rot_key), split_blocks(value), split_blocks(log_decay)))
    retained = retained.reshape(FIRST_POSITIONS, RETENTION_HEADS, VALUE_DIM)
    average = lax.optimization_barrier(jnp.mean(retained, axis=-1, keepdims=True))
    centred = retained - average
    spread = lax.optimization_barrier(jnp.mean(centred * centred, axis=-1, keepdims=True))
    normed_heads = centred * lax.rsqrt(spread + EPSILON) * head_gain.reshape(RETENTION_HEADS, VALUE_DIM).astype(jnp.float32)
    gated = (jax.nn.silu(gate) * normed_heads.reshape(FIRST_POSITIONS, VALUE_WIDTH)).astype(jnp.bfloat16)
    group_cols = VALUE_WIDTH // N_TP
    summed = jnp.zeros((FIRST_POSITIONS, D), jnp.float32)
    for group in range(N_TP):
        lower = group * group_cols
        share_term = jnp.dot(gated[:, lower:lower + group_cols], output_weight[lower:lower + group_cols], preferred_element_type=jnp.float32).astype(jnp.bfloat16)
        summed = summed + share_term.astype(jnp.float32)
    return summed.astype(jnp.bfloat16)

def expert_mixture(expert_input, expert_gain, routes, group_weight, pair_weight, expert_gate, expert_up, expert_down):
    normed = layer_norm(expert_input, expert_gain).astype(jnp.bfloat16)
    flat_routes = routes.reshape(-1).astype(jnp.int32)
    capacity_rows = N_EP * N_TP * CAP
    mixing = (group_weight[:, None] * pair_weight).reshape(-1).astype(jnp.float32)

    def one_expert(carry, expert_id):
        matches = flat_routes == expert_id
        hits = jnp.nonzero(matches, size=capacity_rows, fill_value=0)[0].astype(jnp.int32)
        present = (jnp.arange(capacity_rows) < jnp.sum(matches)).astype(jnp.float32)
        token_ids = (hits // TOPK).astype(jnp.int32)
        gathered = normed[token_ids]
        gate_part = jnp.dot(gathered, expert_gate[expert_id], preferred_element_type=jnp.float32)
        up_part = jnp.dot(gathered, expert_up[expert_id], preferred_element_type=jnp.float32)
        hidden = (jax.nn.silu(gate_part) * up_part).astype(jnp.bfloat16)
        result = jnp.dot(hidden, expert_down[expert_id], preferred_element_type=jnp.float32).astype(jnp.bfloat16)
        contribution = result.astype(jnp.float32) * (mixing[hits] * present)[:, None]
        return (carry.at[token_ids].add(contribution), None)
    total, _ = lax.scan(one_expert, jnp.zeros((TOKENS_B, D), jnp.float32), jnp.arange(EXPERTS, dtype=jnp.int32))
    return total.astype(jnp.bfloat16)

def reference(mixer_input, log_decay, mixer_gain, query_weight, key_weight, value_weight, gate_weight, head_gain, output_weight, expert_input, expert_gain, routes, group_weight, pair_weight, expert_gate, expert_up, expert_down):
    mixer_output = token_mixer(mixer_input, log_decay, mixer_gain, query_weight, key_weight, value_weight, gate_weight, head_gain, output_weight)
    expert_output = expert_mixture(expert_input, expert_gain, routes, group_weight, pair_weight, expert_gate, expert_up, expert_down)
    return (mixer_output, expert_output)
```

```python
import functools

import jax
import jax.numpy as jnp
import numpy as np
from jax import lax
from jax.experimental import pallas as pl
from jax.experimental.pallas import tpu as pltpu
from jax.sharding import PartitionSpec as P

KD = 128
VD = 256
CAP = 3
EPSILON = 1e-05
THETA = 10000.0
CHUNKS = 4
MESH = pl.DeviceIdType.MESH
F32 = jnp.float32
BF16 = jnp.bfloat16
HI = lax.Precision.HIGHEST


def dot(a, b, **kw):
    return jnp.dot(a, b, preferred_element_type=F32, **kw)


def dot_t0(a, b):
    return lax.dot_general(a, b, (((0,), (0,)), ((), ())), preferred_element_type=F32)


def dot_t1(a, b):
    return lax.dot_general(a, b, (((1,), (1,)), ((), ())), preferred_element_type=F32)


def norm_rows(src, gain, dst, rows, step):
    @pl.loop(0, rows // step)
    def _(i):
        at = pl.ds(pl.multiple_of(i * step, step), step)
        m = src[at, :].astype(F32)
        mean = jnp.mean(m, axis=-1, keepdims=True)
        c = m - mean
        var = jnp.mean(c * c, axis=-1, keepdims=True)
        dst[at, :] = (c * lax.rsqrt(var + EPSILON) * gain[...]).astype(BF16)


def rows_of(x3):
    a, b, c = x3.shape
    return x3.astype(F32).reshape(a * b, c).astype(BF16)


def kernel(
    dims,
    x_ref, ld_ref, mgain_ref, wq_ref, wk_ref, wv_ref, wg_ref, hgain_ref, wo_ref,
    e_ref, egain_ref, routes_ref, gw_ref, pw_ref, eg_ref, eu_ref, ed_ref,
    rot_t_ref, rot_b_ref,
    mix_ref, moe_ref,
    w_in, w_out, w_eg, w_eu, w_ed,
    xn, xe, rq, rk, vv, gg, lo, rot_c, rot_s, c_col, c_row,
    sel0, sel1, perm,
    p1s, p1r, p2s, p2r, r1s, r1r, r2s, r2r,
    acc_g, acc_u, hid,
    st_s, st_r, tot_s, tot_r, h_in,
    sib_s, sib_r, own_p, m1_r, m2_s, m2_r,
    wsem, agss, agrs, sbss, sbrs, lsem,
    p1ss, p1rs, p2ss, p2rs, r1ss, r1rs, r2ss, r2rs,
    stss, strs, ttss, ttrs, rsss, rsrs, m1ss, m1rs, m2ss, m2rs,
):
    n_ep, zn, xnn, tok, d, ff = dims
    cw = d // CHUNKS
    slots = n_ep * 8 * CAP
    ep = lax.axis_index("ep")
    tp = lax.axis_index("tp")
    y = tp // 2
    core = tp % 2
    sib = y * 2 + (1 - core)

    def at_y(k):
        return lax.rem(y + k, 4) * 2

    right, left = at_y(1) + core, at_y(3) + core
    order = [(0, 1), (1, 0), (0, 3), (3, 0), (1, 1), (3, 3), (1, 3), (3, 1),
             (2, 0), (0, 2), (1, 2), (3, 2), (2, 1), (2, 3), (2, 2)]
    order = [(a, b) for a, b in order if a < zn and b < xnn]
    n_off = len(order)
    eps = [
        lax.rem(ep // xnn + a, zn) * xnn + lax.rem(ep % xnn + b, xnn) for a, b in order
    ]
    tps = [at_y(a) + lax.rem(core + b, 2)
           for a, b in ((1, 0), (3, 1), (1, 1), (3, 0), (2, 0), (2, 1), (0, 1))]

    loads = [
        pltpu.make_async_copy(wq_ref, w_in.at[:, pl.ds(0, KD)], wsem.at[0]),
        pltpu.make_async_copy(wk_ref, w_in.at[:, pl.ds(KD, KD)], wsem.at[1]),
        pltpu.make_async_copy(wv_ref, w_in.at[:, pl.ds(2 * KD, VD)], wsem.at[2]),
        pltpu.make_async_copy(wg_ref, w_in.at[:, pl.ds(2 * KD + VD, VD)], wsem.at[3]),
        pltpu.make_async_copy(wo_ref, w_out, wsem.at[4]),
        pltpu.make_async_copy(eg_ref, w_eg, wsem.at[5]),
        pltpu.make_async_copy(eu_ref, w_eu, wsem.at[6]),
        pltpu.make_async_copy(ed_ref, w_ed, wsem.at[7]),
    ]
    for c in loads:
        c.start()

    barrier = pltpu.get_barrier_semaphore()
    for t in eps:
        pl.semaphore_signal(barrier, inc=1, device_id={"ep": t}, device_id_type=MESH)
    for t in tps:
        pl.semaphore_signal(barrier, inc=1, device_id={"tp": t}, device_id_type=MESH)

    norm_rows(x_ref, mgain_ref, xn.at[tp], 128, 32)
    pl.semaphore_wait(barrier, n_off + 7)

    def rcopy(src, dst, ss, rs, who):
        return pltpu.make_async_remote_copy(
            src_ref=src, dst_ref=dst, send_sem=ss, recv_sem=rs,
            device_id=who, device_id_type=MESH,
        )

    def ag(direction, piece):
        half = pl.ds(64 * ((piece + direction) % 2), 64)
        if piece == 2:
            half = pl.ds(64 * direction, 64)
            block = left if direction == 0 else right
        else:
            block = tp
        ref = xn.at[block, half]
        return rcopy(ref, ref, agss.at[direction, piece], agrs.at[direction, piece],
                     {"tp": right if direction == 0 else left})

    def ag_in(direction, piece):
        half = pl.ds(64 * ((piece + direction) % 2), 64)
        if piece == 2:
            half = pl.ds(64 * direction, 64)
            block = at_y(2) + core
        else:
            block = left if direction == 0 else right
        ref = xn.at[block, half]
        return rcopy(ref, ref, agss.at[direction, piece], agrs.at[direction, piece],
                     {"tp": right if direction == 0 else left})

    def sb(k, mine=True):
        block = at_y(k) + (core if mine else 1 - core)
        ref = xn.at[block]
        return rcopy(ref, ref, sbss.at[k], sbrs.at[k], {"tp": sib})

    for piece in range(2):
        for direction in range(2):
            ag(direction, piece).start()
    sb(0).start()

    norm_rows(e_ref, egain_ref, xe, tok, min(tok, 32))
    r_io = lax.broadcasted_iota(jnp.int32, (slots, tok), 0)
    group = (r_io * 2731) >> 16
    e_of = group * 8 + (r_io & 7)
    k_of = ((r_io - group * 24) >> 3).astype(F32)
    hit0 = e_of == routes_ref[0:1, :]
    hit1 = e_of == routes_ref[1:2, :]
    hits = jnp.where(jnp.logical_or(hit0, hit1), 1.0, 0.0)
    before = lax.broadcasted_iota(jnp.int32, (tok, tok), 0) < lax.broadcasted_iota(
        jnp.int32, (tok, tok), 1
    )
    rank = dot(hits.astype(BF16), jnp.where(before, 1.0, 0.0).astype(BF16))
    here = jnp.abs(rank - k_of) < 0.5
    s0 = jnp.where(jnp.logical_and(hit0, here), 1.0, 0.0)
    s1 = jnp.where(jnp.logical_and(hit1, here), 1.0, 0.0)
    sel0[...] = s0.astype(BF16)
    sel1[...] = s1.astype(BF16)
    pick = (s0 + s1).astype(BF16)

    def ep_send(buf, into, f, ss, rs):
        for t in eps:
            rcopy(buf.at[f, t], into.at[f, ep], ss.at[f], rs.at[f], {"ep": t}).start()
        pltpu.make_async_copy(buf.at[f, ep], into.at[f, ep], lsem).start()
        pltpu.make_async_copy(buf.at[f, ep], into.at[f, ep], lsem).wait()

    def tp_send(buf, into, f, ss, rs):
        for t in tps:
            rcopy(buf.at[f, t], into.at[f, tp], ss.at[f], rs.at[f], {"tp": t}).start()
        pltpu.make_async_copy(buf.at[f, tp], into.at[f, tp], lsem).start()
        pltpu.make_async_copy(buf.at[f, tp], into.at[f, tp], lsem).wait()

    def all_of(buf, f, n, sem):
        ref = buf.at[f, pl.ds(0, n)]
        return pltpu.make_async_copy(ref, ref, sem.at[f])

    for f in range(CHUNKS):
        part = dot(pick, xe[:, f * cw:(f + 1) * cw])
        p1s[f] = part.reshape(n_ep, 24, cw).astype(BF16)
        ep_send(p1s, p1r, f, p1ss, p1rs)

    upto = lax.broadcasted_iota(jnp.int32, (128, 128), 0) <= lax.broadcasted_iota(
        jnp.int32, (128, 128), 1
    )
    inside = dot(ld_ref[...], jnp.where(upto, 1.0, 0.0), precision=HI)
    run = jnp.zeros((1, 1), F32)
    for b in range(8):
        row = inside[b:b + 1, :] + run
        c_row[b:b + 1, :] = row
        c_col[b] = jnp.transpose(jnp.broadcast_to(row, (128, 128)))
        run = run + inside[b:b + 1, 127:128]
    tot_s[...] = jnp.broadcast_to(run, (8, 128))

    def to_later(make):
        for o, t in enumerate(eps):
            @pl.when(t > ep)
            def _():
                make(o, t).start()

    def st_copy(o, t):
        return rcopy(st_s, st_r.at[ep], stss.at[o], strs.at[o], {"ep": t})

    def tt_copy(o, t):
        return rcopy(tot_s, tot_r.at[ep], ttss.at[o], ttrs.at[o], {"ep": t})

    def back(o):
        a, b = order[o]
        return lax.rem(ep // xnn + zn - a, zn) * xnn + lax.rem(ep % xnn + xnn - b, xnn)

    to_later(tt_copy)

    turn = rot_b_ref[ep]
    cb = turn[:, :KD]
    sbn = turn[:, KD:]
    for i in range(4):
        at = pl.ds(i * 256, 256)
        ct = rot_t_ref[at, :KD]
        st = rot_t_ref[at, KD:]
        rot_c[at, :] = ct * cb - st * sbn
        rot_s[at, :] = st * cb + ct * sbn

    pm_r = lax.broadcasted_iota(jnp.int32, (slots, slots), 0)
    pm_c = lax.broadcasted_iota(jnp.int32, (slots, slots), 1)
    perm[...] = jnp.where(
        pm_r == (pm_c & 7) * (n_ep * CAP) + (pm_c >> 3), 1.0, 0.0
    ).astype(BF16)

    def forward(f):
        all_of(p1r, f, n_off, p1rs).wait()
        moved = dot(perm[...], rows_of(p1r[f])).astype(BF16)
        p2s[f] = moved.reshape(8, n_ep * CAP, cw)
        tp_send(p2s, p2r, f, p2ss, p2rs)

    def project(k):
        first = pl.multiple_of(at_y(k), 2)
        rows = pl.ds(pl.multiple_of(first * 128, 256), 256)
        xb = xn[pl.ds(first, 2)].reshape(256, d)
        cos = rot_c[rows, :]
        sin = rot_s[rows, :]
        qk = dot(xb, w_in[:, :2 * KD])
        for i, ref in enumerate((rq, rk)):
            part = qk[:, i * KD:(i + 1) * KD].astype(BF16).astype(F32)
            ref[rows, :] = (part * cos + pltpu.roll(part, KD // 2, 1) * sin).astype(BF16)
        vv[rows, :] = dot(xb, w_in[:, 2 * KD:2 * KD + VD]).astype(BF16)
        gg[rows, :] = dot(xb, w_in[:, 2 * KD + VD:]).astype(BF16)

    for c in loads[:4]:
        c.wait()
    sb(0, False).wait_recv()
    project(0)
    for direction in range(2):
        ag_in(direction, 0).wait_recv()
        ag(direction, 2).start()
    forward(0)
    for direction in range(2):
        ag_in(direction, 1).wait_recv()
    sb(3).start()
    sb(1).start()
    forward(1)
    sb(3, False).wait_recv()
    project(3)
    sb(1, False).wait_recv()
    project(1)
    forward(2)
    for direction in range(2):
        ag_in(direction, 2).wait_recv()
    sb(2).start()
    forward(3)
    sb(2, False).wait_recv()
    project(2)

    state = jnp.zeros((KD, VD), F32)
    for b in range(4):
        at = pl.ds(b * 256, 256)
        left_over = jnp.exp(run - jnp.concatenate([c_col[2 * b], c_col[2 * b + 1]], axis=0))
        kw = (rk[at, :].astype(F32) * left_over).astype(BF16)
        state = state + dot_t0(kw, vv[at, :])
    st_s[...] = state.astype(BF16)

    causal = lax.broadcasted_iota(jnp.int32, (256, 256), 0) >= lax.broadcasted_iota(
        jnp.int32, (256, 256), 1
    )
    for i in range(4):
        qi = rq[pl.ds(i * 256, 256), :]
        ci = jnp.concatenate([c_col[2 * i], c_col[2 * i + 1]], axis=0)
        ci = jnp.concatenate([ci, ci], axis=1)
        out = jnp.zeros((256, VD), F32)
        for j in range(i + 1):
            at = pl.ds(j * 256, 256)
            cj = jnp.concatenate([c_row[2 * j:2 * j + 1, :], c_row[2 * j + 1:2 * j + 2, :]], axis=1)
            w = jnp.exp(jnp.minimum(ci - cj, 0.0))
            if i == j:
                w = jnp.where(causal, w, 0.0)
            dec = (dot_t1(qi, rk[at, :]) * w).astype(BF16)
            out = out + dot(dec, vv[at, :])
        lo[pl.ds(i * 256, 256), :] = out
        if i == 0:
            to_later(st_copy)

    def expert_in(f):
        all_of(p2r, f, 7, p2rs).wait()
        xf = p2r[f].reshape(slots, cw)

        @pl.loop(0, ff // 256)
        def _(n):
            at = pl.ds(pl.multiple_of(n * 256, 256), 256)
            for acc, w in ((acc_g, w_eg), (acc_u, w_eu)):
                part = dot(xf, w[f * cw:(f + 1) * cw, at])
                if f == 0:
                    acc[:, at] = part
                else:
                    acc[:, at] += part

    for c in loads[5:7]:
        c.wait()
    expert_in(0)
    expert_in(1)

    for o in range(n_off):
        src = back(o)

        @pl.when(src < ep)
        def _():
            rcopy(tot_s, tot_r.at[src], ttss.at[o], ttrs.at[o], {"ep": src}).wait_recv()
            rcopy(st_s, st_r.at[src], stss.at[o], strs.at[o], {"ep": src}).wait_recv()

    after = jnp.zeros((1, 128), F32)
    total = jnp.zeros((KD, VD), F32)
    for e in reversed(range(n_ep)):
        valid = e < ep
        coef = jnp.exp(after)
        part = st_r[e].astype(F32) * jnp.concatenate([coef, coef], axis=1)
        total = total + jnp.where(valid, part, 0.0)
        after = after + jnp.where(valid, tot_r[e, 0:1, :], 0.0)
    h_in[...] = total.astype(BF16)
    loads[4].wait()

    def partial_rows(block):
        at = pl.ds(pl.multiple_of(block * 128, 128), 128)
        col = jnp.exp(c_col[block])
        q = (rq[at, :].astype(F32) * col).astype(BF16)
        ret = lo[at, :] + dot(q, h_in[...])
        mean = jnp.mean(ret, axis=-1, keepdims=True)
        c = ret - mean
        var = jnp.mean(c * c, axis=-1, keepdims=True)
        normed = c * lax.rsqrt(var + EPSILON) * hgain_ref[...]
        g = gg[at, :].astype(F32)
        gated = (g / (1.0 + jnp.exp(-g)) * normed).astype(BF16)
        return gated

    def rs_sib(k):
        return rcopy(sib_s.at[k], sib_r.at[k], rsss.at[k], rsrs.at[k], {"tp": sib})

    def make_partial(k):
        gated = partial_rows(at_y(k) + 1 - core)
        sib_s[k] = dot(gated, w_out[...]).astype(BF16)
        gated = partial_rows(at_y(k) + core)
        rs_sib(k).start()
        own_p[k] = dot(gated, w_out[...])

    def chip_sum(k):
        rs_sib(k).wait_recv()
        return own_p[k] + sib_r[k].astype(F32)

    def m1(direction):
        src = m2_s.at[2, pl.ds(64 * direction, 64)]
        return rcopy(src, m1_r.at[direction], m1ss.at[direction], m1rs.at[direction],
                     {"tp": right if direction == 0 else left})

    def m2(direction, half):
        src = m2_s.at[direction, pl.ds(64 * half, 64)]
        return rcopy(src, m2_r.at[direction, pl.ds(64 * half, 64)],
                     m2ss.at[direction, half], m2rs.at[direction, half],
                     {"tp": right if direction == 0 else left})

    make_partial(2)
    make_partial(1)
    m2_s[2] = chip_sum(2).astype(BF16)
    make_partial(3)
    for direction in range(2):
        m1(direction).start()
    own_p[1] = chip_sum(1)
    m2_s[0, 64:128] = own_p[1, 64:128, :].astype(BF16)
    own_p[3] = chip_sum(3)
    m2_s[1, 0:64] = own_p[3, 0:64, :].astype(BF16)
    make_partial(0)
    m2(0, 1).start()
    m2(1, 0).start()

    expert_in(2)
    for direction in range(2):
        m1(direction).wait_recv()
        half = pl.ds(64 * direction, 64)
        m2_s[direction, half] = (
            own_p[1 if direction == 0 else 3, half, :] + m1_r[direction].astype(F32)
        ).astype(BF16)
    own_p[0] = chip_sum(0)
    for direction in range(2):
        m2(direction, direction).start()

    expert_in(3)

    @pl.loop(0, ff // 256)
    def _(n):
        at = pl.ds(pl.multiple_of(n * 256, 256), 256)
        g = acc_g[:, at]
        hid[:, at] = (g / (1.0 + jnp.exp(-g)) * acc_u[:, at]).astype(BF16)

    loads[7].wait()
    for f in range(CHUNKS):
        part = dot(hid[...], w_ed[:, f * cw:(f + 1) * cw]).astype(BF16)
        r1s[f] = part.reshape(8, n_ep * CAP, cw)
        tp_send(r1s, r1r, f, r1ss, r1rs)
    for f in range(CHUNKS):
        all_of(r1r, f, 7, r1rs).wait()
        moved = dot_t0(perm[...], r1r[f].reshape(slots, cw))
        r2s[f] = moved.reshape(n_ep, 24, cw).astype(BF16)
        ep_send(r2s, r2r, f, r2ss, r2rs)

    for direction in range(2):
        for half in range(2):
            m2(direction, half).wait_recv()
    mix_ref[...] = (
        own_p[0] + m2_r[0].astype(F32) + m2_r[1].astype(F32)
    ).astype(BF16)

    w0 = jnp.transpose(jnp.broadcast_to(gw_ref[...] * pw_ref[0:1, :], (128, tok)))
    w1 = jnp.transpose(jnp.broadcast_to(gw_ref[...] * pw_ref[1:2, :], (128, tok)))
    w0, w1 = w0[:, 0:1], w1[:, 0:1]
    for f in range(CHUNKS):
        all_of(r2r, f, n_off, r2rs).wait()
        got = rows_of(r2r[f])
        moe_ref[:, f * cw:(f + 1) * cw] = (
            w0 * dot_t0(sel0[...], got) + w1 * dot_t0(sel1[...], got)
        ).astype(BF16)

    for direction in range(2):
        for piece in range(3):
            ag(direction, piece).wait_send()
        m1(direction).wait_send()
        for half in range(2):
            m2(direction, half).wait_send()
    for k in range(4):
        sb(k).wait_send()
        rs_sib(k).wait_send()
    for f in range(CHUNKS):
        all_of(p1s, f, n_off, p1ss).wait()
        all_of(p2s, f, 7, p2ss).wait()
        all_of(r1s, f, 7, r1ss).wait()
        all_of(r2s, f, n_off, r2ss).wait()
    for o, t in enumerate(eps):
        @pl.when(t > ep)
        def _():
            tt_copy(o, t).wait_send()
            st_copy(o, t).wait_send()


def rotation_tables(n_ep, rows):
    half = KD // 2
    freq = (THETA ** (-np.arange(half) / half)).astype(np.float32).astype(np.float64)
    sign = np.concatenate([-np.ones(half), np.ones(half)])

    def both(positions):
        angles = np.tile(positions[:, None] * freq[None, :], (1, 2))
        return np.concatenate([np.cos(angles), np.sin(angles) * sign], axis=1)

    inner = both(np.arange(rows, dtype=np.float64))
    outer = both(rows * np.arange(n_ep, dtype=np.float64))
    return inner.astype(np.float32), outer.astype(np.float32)


def solution(mesh):
    n_ep = mesh.shape["ep"]
    zn, xnn = (4, 4) if n_ep == 16 else (n_ep, 1)

    def local(
        mixer_input, log_decay, mixer_gain, query_weight, key_weight, value_weight,
        gate_weight, head_gain, output_weight, expert_input, expert_gain, routes,
        group_weight, pair_weight, expert_gate, expert_up, expert_down,
    ):
        tok, d = expert_input.shape
        ff = expert_gate.shape[2]
        seg = log_decay.shape[0]
        slots = n_ep * 8 * CAP
        cw = d // CHUNKS
        rot_t, rot_b = rotation_tables(n_ep, seg)
        vmem = pl.BlockSpec(memory_space=pltpu.VMEM)
        hbm = pl.BlockSpec(memory_space=pl.ANY)
        in_specs = [vmem, vmem, vmem, hbm, hbm, hbm, hbm, vmem, hbm,
                    vmem, vmem, vmem, vmem, vmem, hbm, hbm, hbm, vmem, vmem]
        V = pltpu.VMEM
        DMA = pltpu.SemaphoreType.DMA
        scratch = [
            V((d, 2 * KD + 2 * VD), BF16), V((VD, d), BF16), V((d, ff), BF16),
            V((d, ff), BF16), V((ff, d), BF16),
            V((8, 128, d), BF16), V((tok, d), BF16), V((seg, KD), BF16), V((seg, KD), BF16),
            V((seg, VD), BF16), V((seg, VD), BF16), V((seg, VD), F32), V((seg, KD), F32),
            V((seg, KD), F32), V((8, 128, 128), F32), V((8, 128), F32),
            V((slots, tok), BF16), V((slots, tok), BF16), V((slots, slots), BF16),
            V((CHUNKS, n_ep, 24, cw), BF16), V((CHUNKS, n_ep, 24, cw), BF16),
            V((CHUNKS, 8, n_ep * CAP, cw), BF16), V((CHUNKS, 8, n_ep * CAP, cw), BF16),
            V((CHUNKS, 8, n_ep * CAP, cw), BF16), V((CHUNKS, 8, n_ep * CAP, cw), BF16),
            V((CHUNKS, n_ep, 24, cw), BF16), V((CHUNKS, n_ep, 24, cw), BF16),
            V((slots, ff), F32), V((slots, ff), F32), V((slots, ff), BF16),
            V((KD, VD), BF16), V((n_ep, KD, VD), BF16), V((8, 128), F32),
            V((n_ep, 8, 128), F32), V((KD, VD), BF16),
            V((4, 128, d), BF16), V((4, 128, d), BF16), V((4, 128, d), F32),
            V((2, 64, d), BF16), V((3, 128, d), BF16), V((2, 128, d), BF16),
            DMA((8,)), DMA((2, 3)), DMA((2, 3)), DMA((4,)), DMA((4,)), DMA,
            DMA((CHUNKS,)), DMA((CHUNKS,)), DMA((CHUNKS,)), DMA((CHUNKS,)),
            DMA((CHUNKS,)), DMA((CHUNKS,)), DMA((CHUNKS,)), DMA((CHUNKS,)),
            DMA((n_ep,)), DMA((n_ep,)), DMA((n_ep,)), DMA((n_ep,)),
            DMA((4,)), DMA((4,)), DMA((2,)), DMA((2,)), DMA((2, 2)), DMA((2, 2)),
        ]
        return pl.pallas_call(
            functools.partial(kernel, (n_ep, zn, xnn, tok, d, ff)),
            out_shape=(
                jax.ShapeDtypeStruct(mixer_input.shape, BF16),
                jax.ShapeDtypeStruct(expert_input.shape, BF16),
            ),
            in_specs=in_specs,
            out_specs=(vmem, vmem),
            scratch_shapes=scratch,
            compiler_params=pltpu.CompilerParams(
                collective_id=0, has_side_effects=True, vmem_limit_bytes=67043328
            ),
        )(
            mixer_input, log_decay.reshape(8, 128), mixer_gain.reshape(1, -1),
            query_weight, key_weight, value_weight, gate_weight,
            head_gain.reshape(1, -1), output_weight, expert_input,
            expert_gain.reshape(1, -1), routes.T, group_weight.reshape(1, -1),
            pair_weight.T, expert_gate[0], expert_up[0], expert_down[0],
            jnp.asarray(rot_t), jnp.asarray(rot_b[:, None, :]),
        )

    return jax.shard_map(
        local,
        mesh=mesh,
        in_specs=(
            P(("ep", "tp"), None), P("ep", "tp"), P(), P(None, "tp"), P(None, "tp"),
            P(None, "tp"), P(None, "tp"), P("tp"), P("tp", None), P(("ep", "tp"), None),
            P(), P(("ep", "tp"), None), P(("ep", "tp")), P(("ep", "tp"), None),
            P(("ep", "tp"), None, None), P(("ep", "tp"), None, None),
            P(("ep", "tp"), None, None),
        ),
        out_specs=(P(("ep", "tp"), None), P(("ep", "tp"), None)),
        check_vma=False,
    )
```

```python
import functools

import jax
import jax.numpy as jnp
import numpy as np
from jax import lax
from jax.experimental import pallas as pl
from jax.experimental.pallas import tpu as pltpu
from jax.sharding import PartitionSpec as P

KD = 128
VD = 256
CAP = 3
EPSILON = 1e-05
THETA = 10000.0
CHUNKS = 4
MESH = pl.DeviceIdType.MESH
F32 = jnp.float32
BF16 = jnp.bfloat16
HI = lax.Precision.HIGHEST


def dot(a, b, **kw):
    return jnp.dot(a, b, preferred_element_type=F32, **kw)


def dot_t0(a, b):
    return lax.dot_general(a, b, (((0,), (0,)), ((), ())), preferred_element_type=F32)


def dot_t1(a, b):
    return lax.dot_general(a, b, (((1,), (1,)), ((), ())), preferred_element_type=F32)


def norm_rows(src, gain, dst, rows, step):
    @pl.loop(0, rows // step)
    def _(i):
        at = pl.ds(pl.multiple_of(i * step, step), step)
        m = src[at, :].astype(F32)
        mean = jnp.mean(m, axis=-1, keepdims=True)
        c = m - mean
        var = jnp.mean(c * c, axis=-1, keepdims=True)
        dst[at, :] = (c * lax.rsqrt(var + EPSILON) * gain[...]).astype(BF16)


def rows_of(x3):
    a, b, c = x3.shape
    return x3.astype(F32).reshape(a * b, c).astype(BF16)


def kernel(
    dims,
    x_ref, ld_ref, mgain_ref, wq_ref, wk_ref, wv_ref, wg_ref, hgain_ref, wo_ref,
    e_ref, egain_ref, routes_ref, gw_ref, pw_ref, eg_ref, eu_ref, ed_ref,
    rot_t_ref, rot_b_ref,
    mix_ref, moe_ref,
    x_v, e_v, rot_v, mix_v, moe_v,
    w_in, w_out, w_eg, w_eu, w_ed,
    xn, xe, rq, rk, vv, gg, lo, rot_c, rot_s, c_col, c_row,
    sel0, sel1, perm,
    p1s, p1r, p2s, p2r, r1s, r1r, r2s, r2r,
    acc_g, acc_u, hid,
    sx_s, sx_r, sz_s, sz_r, tot_s, tot_r, h_in, h_b,
    sib_s, sib_r, own_p, m1_r, m2_s, m2_r,
    wsem, agss, agrs, sbss, sbrs, lsem,
    p1ss, p1rs, p2ss, p2rs, r1ss, r1rs, r2ss, r2rs,
    sxss, sxrs, szss, szrs, ttss, ttrs, osem, rsss, rsrs, m1ss, m1rs, m2ss, m2rs,
):
    n_ep, zn, xnn, tok, d, ff = dims
    cw = d // CHUNKS
    slots = n_ep * 8 * CAP
    ep = lax.axis_index("ep")
    tp = lax.axis_index("tp")
    y = tp // 2
    core = tp % 2
    sib = y * 2 + (1 - core)

    def at_y(k):
        return lax.rem(y + k, 4) * 2

    right, left = at_y(1) + core, at_y(3) + core
    order = [(0, 1), (1, 0), (0, 3), (3, 0), (1, 1), (3, 3), (1, 3), (3, 1),
             (2, 0), (0, 2), (1, 2), (3, 2), (2, 1), (2, 3), (2, 2)]
    order = [(a, b) for a, b in order if a < zn and b < xnn]
    n_off = len(order)
    eps = [
        lax.rem(ep // xnn + a, zn) * xnn + lax.rem(ep % xnn + b, xnn) for a, b in order
    ]
    tps = [at_y(a) + lax.rem(core + b, 2)
           for a, b in ((1, 0), (3, 1), (1, 1), (3, 0), (2, 0), (2, 1), (0, 1))]

    loads = [
        pltpu.make_async_copy(wq_ref, w_in.at[:, pl.ds(0, KD)], wsem.at[0]),
        pltpu.make_async_copy(wk_ref, w_in.at[:, pl.ds(KD, KD)], wsem.at[1]),
        pltpu.make_async_copy(wv_ref, w_in.at[:, pl.ds(2 * KD, VD)], wsem.at[2]),
        pltpu.make_async_copy(wg_ref, w_in.at[:, pl.ds(2 * KD + VD, VD)], wsem.at[3]),
        pltpu.make_async_copy(wo_ref, w_out, wsem.at[4]),
        pltpu.make_async_copy(eg_ref, w_eg, wsem.at[5]),
        pltpu.make_async_copy(eu_ref, w_eu, wsem.at[6]),
        pltpu.make_async_copy(ed_ref, w_ed, wsem.at[7]),
    ]
    first = [
        pltpu.make_async_copy(x_ref, x_v, wsem.at[8]),
        pltpu.make_async_copy(e_ref, e_v, wsem.at[9]),
        pltpu.make_async_copy(rot_t_ref, rot_v, wsem.at[10]),
    ]
    for c in first + loads:
        c.start()

    barrier = pltpu.get_barrier_semaphore()
    for t in eps:
        pl.semaphore_signal(barrier, inc=1, device_id={"ep": t}, device_id_type=MESH)
    for t in tps:
        pl.semaphore_signal(barrier, inc=1, device_id={"tp": t}, device_id_type=MESH)

    first[0].wait()
    norm_rows(x_v, mgain_ref, xn.at[tp], 128, 32)
    pl.semaphore_wait(barrier, n_off + 7)

    def rcopy(src, dst, ss, rs, who):
        return pltpu.make_async_remote_copy(
            src_ref=src, dst_ref=dst, send_sem=ss, recv_sem=rs,
            device_id=who, device_id_type=MESH,
        )

    def ag(direction, piece):
        half = pl.ds(64 * ((piece + direction) % 2), 64)
        if piece == 2:
            half = pl.ds(64 * direction, 64)
            block = left if direction == 0 else right
        else:
            block = tp
        ref = xn.at[block, half]
        return rcopy(ref, ref, agss.at[direction, piece], agrs.at[direction, piece],
                     {"tp": right if direction == 0 else left})

    def ag_in(direction, piece):
        half = pl.ds(64 * ((piece + direction) % 2), 64)
        if piece == 2:
            half = pl.ds(64 * direction, 64)
            block = at_y(2) + core
        else:
            block = left if direction == 0 else right
        ref = xn.at[block, half]
        return rcopy(ref, ref, agss.at[direction, piece], agrs.at[direction, piece],
                     {"tp": right if direction == 0 else left})

    def sb(k, mine=True):
        block = at_y(k) + (core if mine else 1 - core)
        ref = xn.at[block]
        return rcopy(ref, ref, sbss.at[k], sbrs.at[k], {"tp": sib})

    for piece in range(2):
        for direction in range(2):
            ag(direction, piece).start()
    sb(0).start()

    first[1].wait()
    norm_rows(e_v, egain_ref, xe, tok, min(tok, 32))
    r_io = lax.broadcasted_iota(jnp.int32, (slots, tok), 0)
    group = (r_io * 2731) >> 16
    e_of = group * 8 + (r_io & 7)
    k_of = ((r_io - group * 24) >> 3).astype(F32)
    hit0 = e_of == routes_ref[0:1, :]
    hit1 = e_of == routes_ref[1:2, :]
    hits = jnp.where(jnp.logical_or(hit0, hit1), 1.0, 0.0)
    before = lax.broadcasted_iota(jnp.int32, (tok, tok), 0) < lax.broadcasted_iota(
        jnp.int32, (tok, tok), 1
    )
    rank = dot(hits.astype(BF16), jnp.where(before, 1.0, 0.0).astype(BF16))
    here = jnp.abs(rank - k_of) < 0.5
    s0 = jnp.where(jnp.logical_and(hit0, here), 1.0, 0.0)
    s1 = jnp.where(jnp.logical_and(hit1, here), 1.0, 0.0)
    pick = (s0 + s1).astype(BF16)

    def ep_send(buf, into, f, ss, rs):
        for t in eps:
            rcopy(buf.at[f, t], into.at[f, ep], ss.at[f], rs.at[f], {"ep": t}).start()
        pltpu.make_async_copy(buf.at[f, ep], into.at[f, ep], lsem).start()
        pltpu.make_async_copy(buf.at[f, ep], into.at[f, ep], lsem).wait()

    def tp_send(buf, into, f, ss, rs):
        for t in tps:
            rcopy(buf.at[f, t], into.at[f, tp], ss.at[f], rs.at[f], {"tp": t}).start()
        pltpu.make_async_copy(buf.at[f, tp], into.at[f, tp], lsem).start()
        pltpu.make_async_copy(buf.at[f, tp], into.at[f, tp], lsem).wait()

    def all_of(buf, f, n, sem):
        ref = buf.at[f, pl.ds(0, n)]
        return pltpu.make_async_copy(ref, ref, sem.at[f])

    for f in range(CHUNKS):
        part = dot(pick, xe[:, f * cw:(f + 1) * cw])
        p1s[f] = part.reshape(n_ep, 24, cw).astype(BF16)
        ep_send(p1s, p1r, f, p1ss, p1rs)

    upto = lax.broadcasted_iota(jnp.int32, (128, 128), 0) <= lax.broadcasted_iota(
        jnp.int32, (128, 128), 1
    )
    inside = dot(ld_ref[...], jnp.where(upto, 1.0, 0.0), precision=HI)
    run = jnp.zeros((1, 1), F32)
    for b in range(8):
        row = inside[b:b + 1, :] + run
        c_row[b:b + 1, :] = row
        c_col[b] = jnp.transpose(jnp.broadcast_to(row, (128, 128)))
        run = run + inside[b:b + 1, 127:128]
    tot_s[...] = jnp.broadcast_to(run, (8, 128))

    def tt_copy(o):
        return rcopy(tot_s, tot_r.at[ep], ttss.at[o], ttrs.at[o], {"ep": eps[o]})

    def sx_copy(b):
        x_me = ep % xnn
        return rcopy(sx_s, sx_r.at[x_me], sxss.at[b], sxrs.at[b],
                     {"ep": ep - x_me + lax.rem(x_me + b, xnn)})

    def sz_copy(a):
        return rcopy(sz_s, sz_r.at[ep // xnn], szss.at[a], szrs.at[a],
                     {"ep": lax.rem(ep // xnn + a, zn) * xnn + ep % xnn})

    for o in range(n_off):
        tt_copy(o).start()
    tot_r[ep] = tot_s[...]

    first[2].wait()
    turn = rot_b_ref[ep]
    cb = turn[:, :KD]
    sbn = turn[:, KD:]
    for i in range(4):
        at = pl.ds(i * 256, 256)
        ct = rot_v[at, :KD]
        st = rot_v[at, KD:]
        rot_c[at, :] = ct * cb - st * sbn
        rot_s[at, :] = st * cb + ct * sbn

    pm_r = lax.broadcasted_iota(jnp.int32, (slots, slots), 0)
    pm_c = lax.broadcasted_iota(jnp.int32, (slots, slots), 1)
    perm[...] = jnp.where(
        pm_r == (pm_c & 7) * (n_ep * CAP) + (pm_c >> 3), 1.0, 0.0
    ).astype(BF16)

    sel0[...] = dot(perm[...], s0.astype(BF16)).astype(BF16)
    sel1[...] = dot(perm[...], s1.astype(BF16)).astype(BF16)

    def relay(f, got, got_sem, buf, into, ss, rs):
        all_of(got, f, n_off, got_sem).wait()
        moved = dot(perm[...], rows_of(got[f])).astype(BF16)
        buf[f] = moved.reshape(8, n_ep * CAP, cw)
        tp_send(buf, into, f, ss, rs)

    def forward(f):
        relay(f, p1r, p1rs, p2s, p2r, p2ss, p2rs)

    def moe_out(f):
        return pltpu.make_async_copy(
            moe_v.at[f], moe_ref.at[:, pl.ds(f * cw, cw)], osem.at[f])

    def project(k):
        first = pl.multiple_of(at_y(k), 2)
        rows = pl.ds(pl.multiple_of(first * 128, 256), 256)
        xb = xn[pl.ds(first, 2)].reshape(256, d)
        cos = rot_c[rows, :]
        sin = rot_s[rows, :]
        qk = dot(xb, w_in[:, :2 * KD])
        for i, ref in enumerate((rq, rk)):
            part = qk[:, i * KD:(i + 1) * KD].astype(BF16).astype(F32)
            ref[rows, :] = (part * cos + pltpu.roll(part, KD // 2, 1) * sin).astype(BF16)
        vv[rows, :] = dot(xb, w_in[:, 2 * KD:2 * KD + VD]).astype(BF16)
        gg[rows, :] = dot(xb, w_in[:, 2 * KD + VD:]).astype(BF16)

    for c in loads[:4]:
        c.wait()
    sb(0, False).wait_recv()
    project(0)
    for direction in range(2):
        ag_in(direction, 0).wait_recv()
        ag(direction, 2).start()
    forward(0)
    for direction in range(2):
        ag_in(direction, 1).wait_recv()
    sb(3).start()
    sb(1).start()
    forward(1)
    sb(3, False).wait_recv()
    project(3)
    sb(1, False).wait_recv()
    project(1)
    forward(2)
    for direction in range(2):
        ag_in(direction, 2).wait_recv()
    sb(2).start()
    forward(3)
    sb(2, False).wait_recv()
    project(2)

    state = jnp.zeros((KD, VD), F32)
    for b in range(4):
        at = pl.ds(b * 256, 256)
        left_over = jnp.exp(run - jnp.concatenate([c_col[2 * b], c_col[2 * b + 1]], axis=0))
        kw = (rk[at, :].astype(F32) * left_over).astype(BF16)
        state = state + dot_t0(kw, vv[at, :])
    sx_s[...] = state.astype(BF16)
    sx_r[ep % xnn] = state.astype(BF16)

    causal = lax.broadcasted_iota(jnp.int32, (256, 256), 0) >= lax.broadcasted_iota(
        jnp.int32, (256, 256), 1
    )
    for b in range(1, xnn):
        sx_copy(b).start()

    for i in range(4):
        qi = rq[pl.ds(i * 256, 256), :]
        ci = jnp.concatenate([c_col[2 * i], c_col[2 * i + 1]], axis=0)
        ci = jnp.concatenate([ci, ci], axis=1)
        out = jnp.zeros((256, VD), F32)
        for j in range(i + 1):
            at = pl.ds(j * 256, 256)
            cj = jnp.concatenate([c_row[2 * j:2 * j + 1, :], c_row[2 * j + 1:2 * j + 2, :]], axis=1)
            w = jnp.exp(jnp.minimum(ci - cj, 0.0))
            if i == j:
                w = jnp.where(causal, w, 0.0)
            dec = (dot_t1(qi, rk[at, :]) * w).astype(BF16)
            out = out + dot(dec, vv[at, :])
        lo[pl.ds(i * 256, 256), :] = out

    def expert_in(f):
        all_of(p2r, f, 7, p2rs).wait()
        xf = dot_t0(perm[...], p2r[f].reshape(slots, cw)).astype(BF16)

        @pl.loop(0, ff // 256)
        def _(n):
            at = pl.ds(pl.multiple_of(n * 256, 256), 256)
            for acc, w in ((acc_g, w_eg), (acc_u, w_eu)):
                part = dot(xf, w[f * cw:(f + 1) * cw, at])
                if f == 0:
                    acc[:, at] = part
                else:
                    acc[:, at] += part

    for c in loads[5:7]:
        c.wait()
    expert_in(0)

    def lanes(v):
        return jnp.concatenate([v, v], axis=1)

    for o in range(n_off):
        tt_copy(o).wait_recv()
    for b in range(1, xnn):
        sx_copy(b).wait_recv()
    zero = jnp.zeros((1, 128), F32)
    z_me, x_me = ep // xnn, ep % xnn
    row = z_me * xnn
    row_state = jnp.zeros((KD, VD), F32)
    my_state = jnp.zeros((KD, VD), F32)
    row_log, my_log = zero, zero
    for i in reversed(range(xnn)):
        t = tot_r[row + i, 0:1, :]
        part = sx_r[i].astype(F32)
        row_state = row_state + part * lanes(jnp.exp(row_log))
        row_log = row_log + t
        my_state = my_state + jnp.where(i < x_me, part * lanes(jnp.exp(my_log)), 0.0)
        my_log = my_log + jnp.where(i < x_me, t, 0.0)
    sz_s[...] = row_state.astype(BF16)
    sz_r[z_me] = jnp.zeros((KD, VD), BF16)
    h_in[...] = my_state
    for a in range(1, zn):
        sz_copy(a).start()
    expert_in(1)
    for a in range(1, zn):
        sz_copy(a).wait_recv()
    before_rows = jnp.zeros((KD, VD), F32)
    z_log = zero
    for i in reversed(range(zn)):
        t = zero
        for j in range(xnn):
            t = t + tot_r[i * xnn + j, 0:1, :]
        part = sz_r[i].astype(F32) * lanes(jnp.exp(z_log))
        before_rows = before_rows + jnp.where(i < z_me, part, 0.0)
        z_log = z_log + jnp.where(i < z_me, t, 0.0)
    h_b[...] = (h_in[...] + before_rows * lanes(jnp.exp(my_log))).astype(BF16)
    loads[4].wait()

    def partial_rows(block):
        at = pl.ds(pl.multiple_of(block * 128, 128), 128)
        col = jnp.exp(c_col[block])
        q = (rq[at, :].astype(F32) * col).astype(BF16)
        ret = lo[at, :] + dot(q, h_b[...])
        mean = jnp.mean(ret, axis=-1, keepdims=True)
        c = ret - mean
        var = jnp.mean(c * c, axis=-1, keepdims=True)
        normed = c * lax.rsqrt(var + EPSILON) * hgain_ref[...]
        g = gg[at, :].astype(F32)
        return (g / (1.0 + jnp.exp(-g)) * normed).astype(BF16)

    def rs_sib(k):
        return rcopy(sib_s.at[k], sib_r.at[k], rsss.at[k], rsrs.at[k], {"tp": sib})

    def make_partial(k):
        gated = partial_rows(at_y(k) + 1 - core)
        sib_s[k] = dot(gated, w_out[...]).astype(BF16)
        gated = partial_rows(at_y(k) + core)
        rs_sib(k).start()
        own_p[k] = dot(gated, w_out[...])

    def chip_sum(k):
        rs_sib(k).wait_recv()
        return own_p[k] + sib_r[k].astype(F32)

    def m1(direction):
        src = m2_s.at[2, pl.ds(64 * direction, 64)]
        return rcopy(src, m1_r.at[direction], m1ss.at[direction], m1rs.at[direction],
                     {"tp": right if direction == 0 else left})

    def m2(direction, half):
        src = m2_s.at[direction, pl.ds(64 * half, 64)]
        return rcopy(src, m2_r.at[direction, pl.ds(64 * half, 64)],
                     m2ss.at[direction, half], m2rs.at[direction, half],
                     {"tp": right if direction == 0 else left})

    make_partial(2)
    make_partial(1)
    m2_s[2] = chip_sum(2).astype(BF16)
    make_partial(3)
    for direction in range(2):
        m1(direction).start()
    expert_in(2)
    own_p[1] = chip_sum(1)
    m2_s[0, 64:128] = own_p[1, 64:128, :].astype(BF16)
    own_p[3] = chip_sum(3)
    m2_s[1, 0:64] = own_p[3, 0:64, :].astype(BF16)
    expert_in(3)
    m2(0, 1).start()
    m2(1, 0).start()

    @pl.loop(0, ff // 256)
    def _(n):
        at = pl.ds(pl.multiple_of(n * 256, 256), 256)
        g = acc_g[:, at]
        hid[:, at] = (g / (1.0 + jnp.exp(-g)) * acc_u[:, at]).astype(BF16)

    loads[7].wait()
    for f in range(CHUNKS):
        part = dot(hid[...], w_ed[:, f * cw:(f + 1) * cw])
        r1s[f] = part.reshape(n_ep, 24, cw).astype(BF16)
        ep_send(r1s, r1r, f, r1ss, r1rs)

    for direction in range(2):
        m1(direction).wait_recv()
        half = pl.ds(64 * direction, 64)
        m2_s[direction, half] = (
            own_p[1 if direction == 0 else 3, half, :] + m1_r[direction].astype(F32)
        ).astype(BF16)
    w0 = jnp.transpose(jnp.broadcast_to(gw_ref[...] * pw_ref[0:1, :], (128, tok)))
    w1 = jnp.transpose(jnp.broadcast_to(gw_ref[...] * pw_ref[1:2, :], (128, tok)))
    w0, w1 = w0[:, 0:1], w1[:, 0:1]
    for direction in range(2):
        m2(direction, direction).start()
    make_partial(0)
    own_p[0] = chip_sum(0)

    for f in range(CHUNKS):
        relay(f, r1r, r1rs, r2s, r2r, r2ss, r2rs)

    for direction in range(2):
        for half in range(2):
            m2(direction, half).wait_recv()
    mix_v[...] = (
        own_p[0] + m2_r[0].astype(F32) + m2_r[1].astype(F32)
    ).astype(BF16)
    mix_out = pltpu.make_async_copy(mix_v, mix_ref, wsem.at[0])
    mix_out.start()

    for f in range(CHUNKS):
        all_of(r2r, f, 7, r2rs).wait()
        got = r2r[f].reshape(slots, cw)
        moe_v[f] = (
            w0 * dot_t0(sel0[...], got) + w1 * dot_t0(sel1[...], got)
        ).astype(BF16)
        moe_out(f).start()

    for direction in range(2):
        for piece in range(3):
            ag(direction, piece).wait_send()
        m1(direction).wait_send()
        for half in range(2):
            m2(direction, half).wait_send()
    for k in range(4):
        sb(k).wait_send()
        rs_sib(k).wait_send()
    for f in range(CHUNKS):
        all_of(p1s, f, n_off, p1ss).wait()
        all_of(p2s, f, 7, p2ss).wait()
        all_of(r1s, f, n_off, r1ss).wait()
        all_of(r2s, f, 7, r2ss).wait()
    for o in range(n_off):
        tt_copy(o).wait_send()
    for b in range(1, xnn):
        sx_copy(b).wait_send()
    for a in range(1, zn):
        sz_copy(a).wait_send()
    mix_out.wait()
    for f in range(CHUNKS):
        moe_out(f).wait()


def place(a_ref, b_ref, a_out, b_out, buf, in_sem, out_sem):
    parts = 2
    rows = a_ref.shape[0] // parts
    pairs = [(a_ref, a_out, i) for i in range(parts)] + [(b_ref, b_out, i) for i in range(parts)]
    ins = [
        pltpu.make_async_copy(src.at[pl.ds(i * rows, rows)], buf.at[n], in_sem.at[n])
        for n, (src, _, i) in enumerate(pairs)
    ]
    outs = [
        pltpu.make_async_copy(buf.at[n], dst.at[pl.ds(i * rows, rows)], out_sem.at[n])
        for n, (_, dst, i) in enumerate(pairs)
    ]
    for c in ins:
        c.start()
    for c, o in zip(ins, outs):
        c.wait()
        o.start()
    for o in outs:
        o.wait()


def rotation_tables(n_ep, rows):
    half = KD // 2
    freq = (THETA ** (-np.arange(half) / half)).astype(np.float32).astype(np.float64)
    sign = np.concatenate([-np.ones(half), np.ones(half)])

    def both(positions):
        angles = np.tile(positions[:, None] * freq[None, :], (1, 2))
        return np.concatenate([np.cos(angles), np.sin(angles) * sign], axis=1)

    inner = both(np.arange(rows, dtype=np.float64))
    outer = both(rows * np.arange(n_ep, dtype=np.float64))
    return inner.astype(np.float32), outer.astype(np.float32)


def solution(mesh):
    n_ep = mesh.shape["ep"]
    zn, xnn = (4, 4) if n_ep == 16 else (n_ep, 1)

    def local(
        mixer_input, log_decay, mixer_gain, query_weight, key_weight, value_weight,
        gate_weight, head_gain, output_weight, expert_input, expert_gain, routes,
        group_weight, pair_weight, expert_gate, expert_up, expert_down,
    ):
        tok, d = expert_input.shape
        ff = expert_gate.shape[2]
        seg = log_decay.shape[0]
        slots = n_ep * 8 * CAP
        cw = d // CHUNKS
        rot_t, rot_b = rotation_tables(n_ep, seg)
        vmem = pl.BlockSpec(memory_space=pltpu.VMEM)
        hbm = pl.BlockSpec(memory_space=pl.ANY)
        in_specs = [hbm, vmem, vmem, hbm, hbm, hbm, hbm, vmem, hbm,
                    hbm, vmem, vmem, vmem, vmem, hbm, hbm, hbm, hbm, vmem]
        V = pltpu.VMEM
        DMA = pltpu.SemaphoreType.DMA
        scratch = [
            V((128, d), BF16), V((tok, d), BF16), V((seg, 2 * KD), F32), V((128, d), BF16),
            V((CHUNKS, tok, cw), BF16),
            V((d, 2 * KD + 2 * VD), BF16), V((VD, d), BF16), V((d, ff), BF16),
            V((d, ff), BF16), V((ff, d), BF16),
            V((8, 128, d), BF16), V((tok, d), BF16), V((seg, KD), BF16), V((seg, KD), BF16),
            V((seg, VD), BF16), V((seg, VD), BF16), V((seg, VD), F32), V((seg, KD), F32),
            V((seg, KD), F32), V((8, 128, 128), F32), V((8, 128), F32),
            V((slots, tok), BF16), V((slots, tok), BF16), V((slots, slots), BF16),
            V((CHUNKS, n_ep, 24, cw), BF16), V((CHUNKS, n_ep, 24, cw), BF16),
            V((CHUNKS, 8, n_ep * CAP, cw), BF16), V((CHUNKS, 8, n_ep * CAP, cw), BF16),
            V((CHUNKS, n_ep, 24, cw), BF16), V((CHUNKS, n_ep, 24, cw), BF16),
            V((CHUNKS, 8, n_ep * CAP, cw), BF16), V((CHUNKS, 8, n_ep * CAP, cw), BF16),
            V((slots, ff), F32), V((slots, ff), F32), V((slots, ff), BF16),
            V((KD, VD), BF16), V((xnn, KD, VD), BF16), V((KD, VD), BF16), V((zn, KD, VD), BF16),
            V((8, 128), F32), V((n_ep, 8, 128), F32), V((KD, VD), F32), V((KD, VD), BF16),
            V((4, 128, d), BF16), V((4, 128, d), BF16), V((4, 128, d), F32),
            V((2, 64, d), BF16), V((3, 128, d), BF16), V((2, 128, d), BF16),
            DMA((11,)), DMA((2, 3)), DMA((2, 3)), DMA((4,)), DMA((4,)), DMA,
            DMA((CHUNKS,)), DMA((CHUNKS,)), DMA((CHUNKS,)), DMA((CHUNKS,)),
            DMA((CHUNKS,)), DMA((CHUNKS,)), DMA((CHUNKS,)), DMA((CHUNKS,)),
            DMA((xnn,)), DMA((xnn,)), DMA((zn,)), DMA((zn,)), DMA((n_ep,)), DMA((n_ep,)),
            DMA((CHUNKS,)),
            DMA((4,)), DMA((4,)), DMA((2,)), DMA((2,)), DMA((2, 2)), DMA((2, 2)),
        ]
        mixed, moe = pl.pallas_call(
            functools.partial(kernel, (n_ep, zn, xnn, tok, d, ff)),
            out_shape=(
                jax.ShapeDtypeStruct(mixer_input.shape, BF16),
                jax.ShapeDtypeStruct(expert_input.shape, BF16),
            ),
            in_specs=in_specs,
            out_specs=(hbm, hbm),
            scratch_shapes=scratch,
            compiler_params=pltpu.CompilerParams(
                collective_id=0, has_side_effects=True, vmem_limit_bytes=67043328
            ),
        )(
            mixer_input, log_decay.reshape(8, 128), mixer_gain.reshape(1, -1),
            query_weight, key_weight, value_weight, gate_weight,
            head_gain.reshape(1, -1), output_weight, expert_input,
            expert_gain.reshape(1, -1), routes.T, group_weight.reshape(1, -1),
            pair_weight.T, expert_gate[0], expert_up[0], expert_down[0],
            jnp.asarray(rot_t), jnp.asarray(rot_b[:, None, :]),
        )
        rows = mixed.shape[0] // 2
        return pl.pallas_call(
            place,
            out_shape=(
                jax.ShapeDtypeStruct(mixed.shape, BF16),
                jax.ShapeDtypeStruct(moe.shape, BF16),
            ),
            in_specs=[hbm, hbm],
            out_specs=(hbm, hbm),
            scratch_shapes=[V((4, rows, d), BF16), DMA((4,)), DMA((4,))],
        )(mixed, moe)

    return jax.shard_map(
        local,
        mesh=mesh,
        in_specs=(
            P(("ep", "tp"), None), P("ep", "tp"), P(), P(None, "tp"), P(None, "tp"),
            P(None, "tp"), P(None, "tp"), P("tp"), P("tp", None), P(("ep", "tp"), None),
            P(), P(("ep", "tp"), None), P(("ep", "tp")), P(("ep", "tp"), None),
            P(("ep", "tp"), None, None), P(("ep", "tp"), None, None),
            P(("ep", "tp"), None, None),
        ),
        out_specs=(P(("ep", "tp"), None), P(("ep", "tp"), None)),
        check_vma=False,
    )
```

```python
import functools

import jax
import jax.numpy as jnp
import numpy as np
from jax import lax
from jax.experimental import pallas as pl
from jax.experimental.pallas import tpu as pltpu
from jax.sharding import PartitionSpec as P

KD = 128
VD = 256
CAP = 3
EPSILON = 1e-05
THETA = 10000.0
MESH = pl.DeviceIdType.MESH
F32 = jnp.float32
BF16 = jnp.bfloat16
HI = lax.Precision.HIGHEST


def dot(a, b, **kw):
    return jnp.dot(a, b, preferred_element_type=F32, **kw)


def dot_t0(a, b):
    return lax.dot_general(a, b, (((0,), (0,)), ((), ())), preferred_element_type=F32)


def dot_t1(a, b):
    return lax.dot_general(a, b, (((1,), (1,)), ((), ())), preferred_element_type=F32)


def norm_rows(src, gain, dst, start, rows, step):
    @pl.loop(0, rows // step)
    def _(i):
        at = pl.ds(pl.multiple_of(start + i * step, step), step)
        m = src[at, :].astype(F32)
        mean = jnp.mean(m, axis=-1, keepdims=True)
        c = m - mean
        var = jnp.mean(c * c, axis=-1, keepdims=True)
        dst[at, :] = (c * lax.rsqrt(var + EPSILON) * gain[...]).astype(BF16)


def rows_of(x3):
    a, b, c = x3.shape
    return x3.astype(F32).reshape(a * b, c).astype(BF16)


def kernel(
    dims,
    x_ref, ld_in, mgain_in, wq_ref, wk_ref, wv_ref, wg_ref, hgain_in, wo_ref,
    e_ref, egain_in, routes_in, gw_in, pw_in, eg_ref, eu_ref, ed_ref,
    rot_t_ref, rot_b_in,
    mix_ref, moe_ref,
    x_v, e_v, rot_v, mix_v, moe_v,
    ld_ref, mgain_ref, hgain_ref, egain_ref, routes_ref, gw_ref, pw_ref, rot_b_ref,
    w_in, w_out, w_eg, w_eu, w_ed,
    xn, xe, rq, rk, vv, gg, lo, rot_c, rot_s, c_col, c_row,
    sel, perm,
    p1s, p1r, p2s, p2r, r1e, r1er, r1ts, r1tr, r2s, r2r, moe_a, hid,
    sx_s, sx_r, sz_s, sz_r, tot_s, tot_r, h_in, h_b,
    sib_s, sib_r, own_p, m1_r, m2_s, m2_r,
    wsem, agss, agrs, sbss, sbrs, lsem,
    p1ss, p1rs, p2ss, p2rs, r1ss, r1rs, r1tss, r1trs, r2ss, r2rs,
    sxss, sxrs, szss, szrs, ttss, ttrs, rsss, rsrs, m1ss, m1rs, m2ss, m2rs,
):
    n_ep, zn, xnn, tok, d, ff = dims
    slots = n_ep * 8
    ep = lax.axis_index("ep")
    tp = lax.axis_index("tp")
    y = tp // 2
    core = tp % 2
    sib = y * 2 + (1 - core)

    def at_y(k):
        return lax.rem(y + k, 4) * 2

    right, left = at_y(1) + core, at_y(3) + core
    order = [(0, 1), (1, 0), (0, 3), (3, 0), (1, 1), (3, 3), (1, 3), (3, 1),
             (2, 0), (0, 2), (1, 2), (3, 2), (2, 1), (2, 3), (2, 2)]
    order = [(a, b) for a, b in order if a < zn and b < xnn]
    n_off = len(order)
    eps = [
        lax.rem(ep // xnn + a, zn) * xnn + lax.rem(ep % xnn + b, xnn) for a, b in order
    ]
    tps = [at_y(a) + lax.rem(core + b, 2)
           for a, b in ((1, 0), (3, 1), (1, 1), (3, 0), (2, 0), (2, 1), (0, 1))]

    def load(n, src, dst):
        return pltpu.make_async_copy(src, dst, wsem.at[n])

    first = [
        load(8, x_ref.at[pl.ds(0, 64)], x_v.at[pl.ds(0, 64)]),
        load(9, mgain_in, mgain_ref),
        load(10, x_ref.at[pl.ds(64, 64)], x_v.at[pl.ds(64, 64)]),
        load(11, e_ref, e_v),
        load(12, egain_in, egain_ref),
        load(13, routes_in, routes_ref),
        load(14, ld_in, ld_ref),
        load(15, rot_t_ref, rot_v),
        load(16, rot_b_in.at[ep], rot_b_ref),
        load(17, hgain_in, hgain_ref),
        load(18, gw_in, gw_ref),
        load(19, pw_in, pw_ref),
    ]
    loads = [
        pltpu.make_async_copy(wq_ref, w_in.at[:, pl.ds(0, KD)], wsem.at[0]),
        pltpu.make_async_copy(wk_ref, w_in.at[:, pl.ds(KD, KD)], wsem.at[1]),
        pltpu.make_async_copy(wv_ref, w_in.at[:, pl.ds(2 * KD, VD)], wsem.at[2]),
        pltpu.make_async_copy(wg_ref, w_in.at[:, pl.ds(2 * KD + VD, VD)], wsem.at[3]),
        pltpu.make_async_copy(wo_ref, w_out, wsem.at[4]),
        pltpu.make_async_copy(eg_ref, w_eg, wsem.at[5]),
        pltpu.make_async_copy(eu_ref, w_eu, wsem.at[6]),
        pltpu.make_async_copy(ed_ref, w_ed, wsem.at[7]),
    ]
    for c in first[:3]:
        c.start()

    barrier = pltpu.get_barrier_semaphore()
    for t in tps:
        pl.semaphore_signal(barrier, inc=1, device_id={"tp": t}, device_id_type=MESH)
    for t in eps:
        pl.semaphore_signal(barrier, inc=1, device_id={"ep": t}, device_id_type=MESH)
    for c in first[3:] + loads:
        c.start()

    for c in first[:2]:
        c.wait()
    norm_rows(x_v, mgain_ref, xn.at[tp], 0, 64, 32)
    first[2].wait()
    norm_rows(x_v, mgain_ref, xn.at[tp], 64, 64, 32)
    pl.semaphore_wait(barrier, n_off + 7)

    def rcopy(src, dst, ss, rs, who):
        return pltpu.make_async_remote_copy(
            src_ref=src, dst_ref=dst, send_sem=ss, recv_sem=rs,
            device_id=who, device_id_type=MESH,
        )

    def ag(direction, piece):
        half = pl.ds(64 * ((piece + direction) % 2), 64)
        if piece == 2:
            half = pl.ds(64 * direction, 64)
            block = left if direction == 0 else right
        else:
            block = tp
        ref = xn.at[block, half]
        return rcopy(ref, ref, agss.at[direction, piece], agrs.at[direction, piece],
                     {"tp": right if direction == 0 else left})

    def ag_in(direction, piece):
        half = pl.ds(64 * ((piece + direction) % 2), 64)
        if piece == 2:
            half = pl.ds(64 * direction, 64)
            block = at_y(2) + core
        else:
            block = left if direction == 0 else right
        ref = xn.at[block, half]
        return rcopy(ref, ref, agss.at[direction, piece], agrs.at[direction, piece],
                     {"tp": right if direction == 0 else left})

    def sb_half(half, mine=True):
        block = at_y(2) + (core if mine else 1 - core)
        ref = xn.at[block, pl.ds(64 * half, 64)]
        return rcopy(ref, ref, sbss.at[2 + 2 * half], sbrs.at[2 + 2 * half], {"tp": sib})

    def sb(k, mine=True):
        block = at_y(k) + (core if mine else 1 - core)
        ref = xn.at[block]
        return rcopy(ref, ref, sbss.at[k], sbrs.at[k], {"tp": sib})

    for piece in range(2):
        for direction in range(2):
            ag(direction, piece).start()
    sb(0).start()

    for c in first[3:6]:
        c.wait()
    norm_rows(e_v, egain_ref, xe, 0, tok, min(tok, 32))
    e_of = lax.broadcasted_iota(jnp.int32, (slots, tok), 0)
    hit0 = e_of == routes_ref[0:1, :]
    hit1 = e_of == routes_ref[1:2, :]
    hits = jnp.where(jnp.logical_or(hit0, hit1), 1.0, 0.0)
    before = lax.broadcasted_iota(jnp.int32, (tok, tok), 0) < lax.broadcasted_iota(
        jnp.int32, (tok, tok), 1
    )
    rank = dot(hits.astype(BF16), jnp.where(before, 1.0, 0.0).astype(BF16))

    def ep_send(buf, into, f, ss, rs):
        for t in eps:
            rcopy(buf.at[f, t], into.at[f, ep], ss.at[f], rs.at[f], {"ep": t}).start()
        pltpu.make_async_copy(buf.at[f, ep], into.at[f, ep], lsem).start()
        pltpu.make_async_copy(buf.at[f, ep], into.at[f, ep], lsem).wait()

    def tp_send(buf, into, f, ss, rs):
        for t in tps:
            rcopy(buf.at[f, t], into.at[f, tp], ss.at[f], rs.at[f], {"tp": t}).start()
        pltpu.make_async_copy(buf.at[f, tp], into.at[f, tp], lsem).start()
        pltpu.make_async_copy(buf.at[f, tp], into.at[f, tp], lsem).wait()

    def all_of(buf, f, n, sem):
        ref = buf.at[f, pl.ds(0, n)]
        return pltpu.make_async_copy(ref, ref, sem.at[f])

    for k in range(CAP):
        here = jnp.abs(rank - float(k)) < 0.5
        s0 = jnp.where(jnp.logical_and(hit0, here), 1.0, 0.0)
        s1 = jnp.where(jnp.logical_and(hit1, here), 1.0, 0.0)
        sel[k, 0] = s0.astype(BF16)
        sel[k, 1] = s1.astype(BF16)
        part = dot((s0 + s1).astype(BF16), xe[...])
        p1s[k] = part.reshape(n_ep, 8, d).astype(BF16)
        ep_send(p1s, p1r, k, p1ss, p1rs)

    for c in first[6:]:
        c.wait()
    upto = lax.broadcasted_iota(jnp.int32, (128, 128), 0) <= lax.broadcasted_iota(
        jnp.int32, (128, 128), 1
    )
    inside = dot(ld_ref[...], jnp.where(upto, 1.0, 0.0), precision=HI)
    run = jnp.zeros((1, 1), F32)
    for b in range(8):
        row = inside[b:b + 1, :] + run
        c_row[b:b + 1, :] = row
        c_col[b] = jnp.transpose(jnp.broadcast_to(row, (128, 128)))
        run = run + inside[b:b + 1, 127:128]
    tot_s[...] = jnp.broadcast_to(run, (8, 128))

    def tt_copy(o):
        return rcopy(tot_s, tot_r.at[ep], ttss.at[o], ttrs.at[o], {"ep": eps[o]})

    def sx_copy(b):
        x_me = ep % xnn
        return rcopy(sx_s, sx_r.at[x_me], sxss.at[b], sxrs.at[b],
                     {"ep": ep - x_me + lax.rem(x_me + b, xnn)})

    def sz_copy(a):
        return rcopy(sz_s, sz_r.at[ep // xnn], szss.at[a], szrs.at[a],
                     {"ep": lax.rem(ep // xnn + a, zn) * xnn + ep % xnn})

    for o in range(n_off):
        tt_copy(o).start()
    tot_r[ep] = tot_s[...]

    turn = rot_b_ref[...]
    cb = turn[:, :KD]
    sbn = turn[:, KD:]
    for i in range(4):
        at = pl.ds(i * 256, 256)
        ct = rot_v[at, :KD]
        st = rot_v[at, KD:]
        rot_c[at, :] = ct * cb - st * sbn
        rot_s[at, :] = st * cb + ct * sbn

    pm_r = lax.broadcasted_iota(jnp.int32, (slots, slots), 0)
    pm_c = lax.broadcasted_iota(jnp.int32, (slots, slots), 1)
    perm[...] = jnp.where(
        pm_r == (pm_c & 7) * n_ep + (pm_c >> 3), 1.0, 0.0
    ).astype(BF16)

    for k in range(1, CAP):
        for j in range(2):
            sel[k, j] = dot(perm[...], sel[k, j]).astype(BF16)

    def relay(f, got, got_sem, buf, into, ss, rs):
        all_of(got, f, n_off, got_sem).wait()
        moved = dot(perm[...], rows_of(got[f])).astype(BF16)
        buf[f] = moved.reshape(8, n_ep, d)
        tp_send(buf, into, f, ss, rs)

    def forward(f):
        relay(f, p1r, p1rs, p2s, p2r, p2ss, p2rs)

    def project(first, count):
        rows = pl.ds(pl.multiple_of(first * 128, 128), count * 128)
        xb = xn[pl.ds(first, count)].reshape(count * 128, d)
        cos = rot_c[rows, :]
        sin = rot_s[rows, :]
        qk = dot(xb, w_in[:, :2 * KD])
        for i, ref in enumerate((rq, rk)):
            part = qk[:, i * KD:(i + 1) * KD].astype(BF16).astype(F32)
            ref[rows, :] = (part * cos + pltpu.roll(part, KD // 2, 1) * sin).astype(BF16)
        vv[rows, :] = dot(xb, w_in[:, 2 * KD:2 * KD + VD]).astype(BF16)
        gg[rows, :] = dot(xb, w_in[:, 2 * KD + VD:]).astype(BF16)

    def state_of(part):
        total = jnp.zeros((KD, VD), F32)
        for k in ((0,), (1, 3), (2,))[part]:
            first = at_y(k)
            at = pl.ds(pl.multiple_of(first * 128, 256), 256)
            left_over = jnp.exp(run - c_col[pl.ds(first, 2)].reshape(256, 128))
            kw = (rk[at, :].astype(F32) * left_over).astype(BF16)
            total = total + dot_t0(kw, vv[at, :])
        return total

    for c in loads[:4]:
        c.wait()
    sb(0, False).wait_recv()
    project(at_y(0), 2)
    for direction in range(2):
        ag_in(direction, 0).wait_recv()
        ag(direction, 2).start()
    forward(0)
    for direction in range(2):
        ag_in(direction, 1).wait_recv()
    sb(3).start()
    sb(1).start()
    forward(1)
    sb(3, False).wait_recv()
    project(at_y(3), 2)
    sb(1, False).wait_recv()
    project(at_y(1), 2)
    for direction in range(2):
        ag_in(direction, 2).wait_recv()
        sb_half(direction).start()
    state = state_of(0) + state_of(1)
    project(at_y(2) + core, 1)
    for direction in range(2):
        sb_half(direction, False).wait_recv()
    project(at_y(2) + 1 - core, 1)

    state = state + state_of(2)
    sx_s[...] = state.astype(BF16)
    sx_r[ep % xnn] = state.astype(BF16)

    causal = lax.broadcasted_iota(jnp.int32, (256, 256), 0) >= lax.broadcasted_iota(
        jnp.int32, (256, 256), 1
    )
    for b in range(1, xnn):
        sx_copy(b).start()
    forward(2)

    for i in range(4):
        qi = rq[pl.ds(i * 256, 256), :]
        ci = jnp.concatenate([c_col[2 * i], c_col[2 * i + 1]], axis=0)
        ci = jnp.concatenate([ci, ci], axis=1)
        out = jnp.zeros((256, VD), F32)
        for j in range(i + 1):
            at = pl.ds(j * 256, 256)
            cj = jnp.concatenate([c_row[2 * j:2 * j + 1, :], c_row[2 * j + 1:2 * j + 2, :]], axis=1)
            w = jnp.exp(jnp.minimum(ci - cj, 0.0))
            if i == j:
                w = jnp.where(causal, w, 0.0)
            dec = (dot_t1(qi, rk[at, :]) * w).astype(BF16)
            out = out + dot(dec, vv[at, :])
        lo[pl.ds(i * 256, 256), :] = out

    def expert_in(k):
        all_of(p2r, k, 7, p2rs).wait()
        xk = p2r[k].reshape(slots, d)

        @pl.loop(0, ff // 256)
        def _(n):
            at = pl.ds(pl.multiple_of(n * 256, 256), 256)
            g = dot(xk, w_eg[:, at])
            u = dot(xk, w_eu[:, at])
            hid[:, at] = (g / (1.0 + jnp.exp(-g)) * u).astype(BF16)

    def expert_out(k, along_tp):
        h = hid[...] if along_tp else dot_t0(perm[...], hid[...]).astype(BF16)
        for n in range(4):
            at = pl.ds(n * (d // 4), d // 4)
            part = dot(h, w_ed[:, n * (d // 4):(n + 1) * (d // 4)])
            if along_tp:
                r1ts[0, :, :, at] = part.astype(BF16).reshape(8, n_ep, d // 4)
            else:
                r1e[k, :, :, at] = part.reshape(n_ep, 8, d // 4).astype(BF16)

    for c in loads[4:]:
        c.wait()
    expert_in(0)

    def lanes(v):
        return jnp.concatenate([v, v], axis=1)

    for o in range(n_off):
        tt_copy(o).wait_recv()
    for b in range(1, xnn):
        sx_copy(b).wait_recv()
    zero = jnp.zeros((1, 128), F32)
    z_me, x_me = ep // xnn, ep % xnn
    row = z_me * xnn
    row_state = jnp.zeros((KD, VD), F32)
    my_state = jnp.zeros((KD, VD), F32)
    row_log, my_log = zero, zero
    for i in reversed(range(xnn)):
        t = tot_r[row + i, 0:1, :]
        part = sx_r[i].astype(F32)
        row_state = row_state + part * lanes(jnp.exp(row_log))
        row_log = row_log + t
        my_state = my_state + jnp.where(i < x_me, part * lanes(jnp.exp(my_log)), 0.0)
        my_log = my_log + jnp.where(i < x_me, t, 0.0)
    sz_s[...] = row_state.astype(BF16)
    sz_r[z_me] = jnp.zeros((KD, VD), BF16)
    h_in[...] = my_state
    for a in range(1, zn):
        sz_copy(a).start()
    expert_out(0, True)
    tp_send(r1ts, r1tr, 0, r1tss, r1trs)
    expert_in(1)
    expert_out(1, False)
    ep_send(r1e, r1er, 1, r1ss, r1rs)
    for a in range(1, zn):
        sz_copy(a).wait_recv()
    before_rows = jnp.zeros((KD, VD), F32)
    z_log = zero
    for i in reversed(range(zn)):
        t = zero
        for j in range(xnn):
            t = t + tot_r[i * xnn + j, 0:1, :]
        part = sz_r[i].astype(F32) * lanes(jnp.exp(z_log))
        before_rows = before_rows + jnp.where(i < z_me, part, 0.0)
        z_log = z_log + jnp.where(i < z_me, t, 0.0)
    h_b[...] = (h_in[...] + before_rows * lanes(jnp.exp(my_log))).astype(BF16)

    def partial_rows(block):
        at = pl.ds(pl.multiple_of(block * 128, 128), 128)
        col = jnp.exp(c_col[block])
        q = (rq[at, :].astype(F32) * col).astype(BF16)
        ret = lo[at, :] + dot(q, h_b[...])
        mean = jnp.mean(ret, axis=-1, keepdims=True)
        c = ret - mean
        var = jnp.mean(c * c, axis=-1, keepdims=True)
        normed = c * lax.rsqrt(var + EPSILON) * hgain_ref[...]
        g = gg[at, :].astype(F32)
        return (g / (1.0 + jnp.exp(-g)) * normed).astype(BF16)

    def relay_ep():
        all_of(r1tr, 0, 7, r1trs).wait()
        moved = dot_t0(perm[...], r1tr[0].reshape(slots, d))
        r1e[0] = moved.reshape(n_ep, 8, d).astype(BF16)
        ep_send(r1e, r1er, 0, r1ss, r1rs)

    def rs_sib(k):
        return rcopy(sib_s.at[k], sib_r.at[k], rsss.at[k], rsrs.at[k], {"tp": sib})

    def sib_part(k):
        gated = partial_rows(at_y(k) + 1 - core)
        sib_s[k] = dot(gated, w_out[...]).astype(BF16)

    def own_part(k):
        gated = partial_rows(at_y(k) + core)
        rs_sib(k).start()
        own_p[k] = dot(gated, w_out[...])

    def chip_sum(k):
        rs_sib(k).wait_recv()
        return own_p[k] + sib_r[k].astype(F32)

    def m1(direction):
        src = m2_s.at[2, pl.ds(64 * direction, 64)]
        return rcopy(src, m1_r.at[direction], m1ss.at[direction], m1rs.at[direction],
                     {"tp": right if direction == 0 else left})

    def m2(direction, half):
        src = m2_s.at[direction, pl.ds(64 * half, 64)]
        return rcopy(src, m2_r.at[direction, pl.ds(64 * half, 64)],
                     m2ss.at[direction, half], m2rs.at[direction, half],
                     {"tp": right if direction == 0 else left})

    sib_part(2)
    own_part(2)
    sib_part(1)
    m2_s[2] = chip_sum(2).astype(BF16)
    own_part(1)
    for direction in range(2):
        m1(direction).start()
    expert_in(2)
    expert_out(2, False)
    own_p[1] = chip_sum(1)
    m2_s[0, 64:128] = own_p[1, 64:128, :].astype(BF16)
    ep_send(r1e, r1er, 2, r1ss, r1rs)
    sib_part(3)
    own_part(3)
    m2(0, 1).start()
    relay_ep()
    own_p[3] = chip_sum(3)
    m2_s[1, 0:64] = own_p[3, 0:64, :].astype(BF16)
    relay(1, r1er, r1rs, r2s, r2r, r2ss, r2rs)
    m2(1, 0).start()
    sib_part(0)
    own_part(0)

    for direction in range(2):
        m1(direction).wait_recv()
        half = pl.ds(64 * direction, 64)
        m2_s[direction, half] = (
            own_p[1 if direction == 0 else 3, half, :] + m1_r[direction].astype(F32)
        ).astype(BF16)
    w0 = jnp.transpose(jnp.broadcast_to(gw_ref[...] * pw_ref[0:1, :], (128, tok)))
    w1 = jnp.transpose(jnp.broadcast_to(gw_ref[...] * pw_ref[1:2, :], (128, tok)))
    w0, w1 = w0[:, 0:1], w1[:, 0:1]
    for direction in range(2):
        m2(direction, direction).start()
    relay(2, r1er, r1rs, r2s, r2r, r2ss, r2rs)

    def combine(k, got):
        for n in range(4):
            at = pl.ds(n * (d // 4), d // 4)
            part = w0 * dot_t0(sel[k, 0], got[:, n * (d // 4):(n + 1) * (d // 4)])
            part = part + w1 * dot_t0(sel[k, 1], got[:, n * (d // 4):(n + 1) * (d // 4)])
            if k == 0:
                moe_a[:, at] = part
            elif k == 1:
                moe_a[:, at] += part
            else:
                moe_v[:, at] = (moe_a[:, at] + part).astype(BF16)

    all_of(r1er, 0, n_off, r1rs).wait()
    combine(0, rows_of(r1er[0]))
    for direction in range(2):
        for half in range(2):
            m2(direction, half).wait_recv()
    mix_v[...] = (
        chip_sum(0) + m2_r[0].astype(F32) + m2_r[1].astype(F32)
    ).astype(BF16)
    mix_out = pltpu.make_async_copy(mix_v, mix_ref, wsem.at[0])
    mix_out.start()

    for k in range(1, CAP):
        all_of(r2r, k, 7, r2rs).wait()
        combine(k, r2r[k].reshape(slots, d))
    moe_out = pltpu.make_async_copy(moe_v, moe_ref, wsem.at[1])
    moe_out.start()

    for direction in range(2):
        for piece in range(3):
            ag(direction, piece).wait_send()
        m1(direction).wait_send()
        for half in range(2):
            m2(direction, half).wait_send()
    for k in range(4):
        rs_sib(k).wait_send()
    for k in (0, 1, 3):
        sb(k).wait_send()
    for half in range(2):
        sb_half(half).wait_send()
    for k in range(CAP):
        all_of(p1s, k, n_off, p1ss).wait()
        all_of(p2s, k, 7, p2ss).wait()
        all_of(r1e, k, n_off, r1ss).wait()
        if k:
            all_of(r2s, k, 7, r2ss).wait()
    all_of(r1ts, 0, 7, r1tss).wait()
    for o in range(n_off):
        tt_copy(o).wait_send()
    for b in range(1, xnn):
        sx_copy(b).wait_send()
    for a in range(1, zn):
        sz_copy(a).wait_send()
    mix_out.wait()
    moe_out.wait()


def place(a_ref, b_ref, a_out, b_out, buf, in_sem, out_sem):
    parts = 2
    rows = a_ref.shape[0] // parts
    pairs = [(a_ref, a_out, i) for i in range(parts)] + [(b_ref, b_out, i) for i in range(parts)]
    ins = [
        pltpu.make_async_copy(src.at[pl.ds(i * rows, rows)], buf.at[n], in_sem.at[n])
        for n, (src, _, i) in enumerate(pairs)
    ]
    outs = [
        pltpu.make_async_copy(buf.at[n], dst.at[pl.ds(i * rows, rows)], out_sem.at[n])
        for n, (_, dst, i) in enumerate(pairs)
    ]
    for c in ins:
        c.start()
    for c, o in zip(ins, outs):
        c.wait()
        o.start()
    for o in outs:
        o.wait()


def rotation_tables(n_ep, rows):
    half = KD // 2
    freq = (THETA ** (-np.arange(half) / half)).astype(np.float32).astype(np.float64)
    sign = np.concatenate([-np.ones(half), np.ones(half)])

    def both(positions):
        angles = np.tile(positions[:, None] * freq[None, :], (1, 2))
        return np.concatenate([np.cos(angles), np.sin(angles) * sign], axis=1)

    inner = both(np.arange(rows, dtype=np.float64))
    outer = both(rows * np.arange(n_ep, dtype=np.float64))
    return inner.astype(np.float32), outer.astype(np.float32)


def solution(mesh):
    n_ep = mesh.shape["ep"]
    zn, xnn = (4, 4) if n_ep == 16 else (n_ep, 1)

    def local(
        mixer_input, log_decay, mixer_gain, query_weight, key_weight, value_weight,
        gate_weight, head_gain, output_weight, expert_input, expert_gain, routes,
        group_weight, pair_weight, expert_gate, expert_up, expert_down,
    ):
        tok, d = expert_input.shape
        ff = expert_gate.shape[2]
        seg = log_decay.shape[0]
        slots = n_ep * 8
        rot_t, rot_b = rotation_tables(n_ep, seg)
        hbm = pl.BlockSpec(memory_space=pl.ANY)
        in_specs = [hbm] * 19
        V = pltpu.VMEM
        DMA = pltpu.SemaphoreType.DMA
        scratch = [
            V((128, d), BF16), V((tok, d), BF16), V((seg, 2 * KD), F32), V((128, d), BF16),
            V((tok, d), BF16),
            V((8, 128), F32), V((1, d), F32), V((1, VD), F32), V((1, d), F32),
            V((2, tok), jnp.int32), V((1, tok), F32), V((2, tok), F32), V((1, 2 * KD), F32),
            V((d, 2 * KD + 2 * VD), BF16), V((VD, d), BF16), V((d, ff), BF16),
            V((d, ff), BF16), V((ff, d), BF16),
            V((8, 128, d), BF16), V((tok, d), BF16), V((seg, KD), BF16), V((seg, KD), BF16),
            V((seg, VD), BF16), V((seg, VD), BF16), V((seg, VD), F32), V((seg, KD), F32),
            V((seg, KD), F32), V((8, 128, 128), F32), V((8, 128), F32),
            V((CAP, 2, slots, tok), BF16), V((slots, slots), BF16),
            V((CAP, n_ep, 8, d), BF16), V((CAP, n_ep, 8, d), BF16),
            V((CAP, 8, n_ep, d), BF16), V((CAP, 8, n_ep, d), BF16),
            V((CAP, n_ep, 8, d), BF16), V((CAP, n_ep, 8, d), BF16),
            V((1, 8, n_ep, d), BF16), V((1, 8, n_ep, d), BF16),
            V((CAP, 8, n_ep, d), BF16), V((CAP, 8, n_ep, d), BF16),
            V((tok, d), F32), V((slots, ff), BF16),
            V((KD, VD), BF16), V((xnn, KD, VD), BF16), V((KD, VD), BF16), V((zn, KD, VD), BF16),
            V((8, 128), F32), V((n_ep, 8, 128), F32), V((KD, VD), F32), V((KD, VD), BF16),
            V((4, 128, d), BF16), V((4, 128, d), BF16), V((4, 128, d), F32),
            V((2, 64, d), BF16), V((3, 128, d), BF16), V((2, 128, d), BF16),
            DMA((20,)), DMA((2, 3)), DMA((2, 3)), DMA((5,)), DMA((5,)), DMA,
            DMA((CAP,)), DMA((CAP,)), DMA((CAP,)), DMA((CAP,)), DMA((CAP,)), DMA((CAP,)),
            DMA((1,)), DMA((1,)), DMA((CAP,)), DMA((CAP,)),
            DMA((xnn,)), DMA((xnn,)), DMA((zn,)), DMA((zn,)), DMA((n_ep,)), DMA((n_ep,)),
            DMA((4,)), DMA((4,)), DMA((2,)), DMA((2,)), DMA((2, 2)), DMA((2, 2)),
        ]
        mixed, moe = pl.pallas_call(
            functools.partial(kernel, (n_ep, zn, xnn, tok, d, ff)),
            out_shape=(
                jax.ShapeDtypeStruct(mixer_input.shape, BF16),
                jax.ShapeDtypeStruct(expert_input.shape, BF16),
            ),
            in_specs=in_specs,
            out_specs=(hbm, hbm),
            scratch_shapes=scratch,
            compiler_params=pltpu.CompilerParams(
                collective_id=0, has_side_effects=True, vmem_limit_bytes=67043328
            ),
        )(
            mixer_input, log_decay.reshape(8, 128), mixer_gain.reshape(1, -1),
            query_weight, key_weight, value_weight, gate_weight,
            head_gain.reshape(1, -1), output_weight, expert_input,
            expert_gain.reshape(1, -1), routes.T, group_weight.reshape(1, -1),
            pair_weight.T, expert_gate[0], expert_up[0], expert_down[0],
            jnp.asarray(rot_t), jnp.asarray(rot_b[:, None, :]),
        )
        rows = mixed.shape[0] // 2
        return pl.pallas_call(
            place,
            out_shape=(
                jax.ShapeDtypeStruct(mixed.shape, BF16),
                jax.ShapeDtypeStruct(moe.shape, BF16),
            ),
            in_specs=[hbm, hbm],
            out_specs=(hbm, hbm),
            scratch_shapes=[V((4, rows, d), BF16), DMA((4,)), DMA((4,))],
        )(mixed, moe)

    return jax.shard_map(
        local,
        mesh=mesh,
        in_specs=(
            P(("ep", "tp"), None), P("ep", "tp"), P(), P(None, "tp"), P(None, "tp"),
            P(None, "tp"), P(None, "tp"), P("tp"), P("tp", None), P(("ep", "tp"), None),
            P(), P(("ep", "tp"), None), P(("ep", "tp")), P(("ep", "tp"), None),
            P(("ep", "tp"), None, None), P(("ep", "tp"), None, None),
            P(("ep", "tp"), None, None),
        ),
        out_specs=(P(("ep", "tp"), None), P(("ep", "tp"), None)),
        check_vma=False,
    )
```

```python
import functools

import jax
import jax.numpy as jnp
import numpy as np
from jax import lax
from jax.experimental import pallas as pl
from jax.experimental.pallas import tpu as pltpu
from jax.sharding import PartitionSpec as P

KD = 128
VD = 256
CAP = 3
EPSILON = 1e-05
THETA = 10000.0
MESH = pl.DeviceIdType.MESH
F32 = jnp.float32
BF16 = jnp.bfloat16
HI = lax.Precision.HIGHEST


def dot(a, b, **kw):
    return jnp.dot(a, b, preferred_element_type=F32, **kw)


def dot_t0(a, b):
    return lax.dot_general(a, b, (((0,), (0,)), ((), ())), preferred_element_type=F32)


def dot_t1(a, b):
    return lax.dot_general(a, b, (((1,), (1,)), ((), ())), preferred_element_type=F32)


def norm_rows(src, gain, dst, start, rows, step):
    @pl.loop(0, rows // step)
    def _(i):
        at = pl.ds(pl.multiple_of(start + i * step, step), step)
        m = src[at, :].astype(F32)
        mean = jnp.mean(m, axis=-1, keepdims=True)
        c = m - mean
        var = jnp.mean(c * c, axis=-1, keepdims=True)
        dst[at, :] = (c * lax.rsqrt(var + EPSILON) * gain[...]).astype(BF16)


def rows_of(x3):
    a, b, c = x3.shape
    return x3.astype(F32).reshape(a * b, c).astype(BF16)


def kernel(
    dims,
    x_ref, ld_in, mgain_in, wq_ref, wk_ref, wv_ref, wg_ref, hgain_in, wo_ref,
    e_ref, egain_in, routes_in, gw_in, pw_in, eg_ref, eu_ref, ed_ref,
    rot_t_ref, rot_b_in,
    mix_ref, moe_ref,
    x_v, e_v, rot_v,
    ld_ref, mgain_ref, hgain_ref, egain_ref, routes_ref, gw_ref, pw_ref, rot_b_ref,
    w_in, w_out, w_eg, w_eu, w_ed,
    xn, xe, rq, rk, vv, gg, lo, rot_c, rot_s, c_col, c_row,
    sel, perm,
    p1s, p1r, p2s, p2r, r1e, r1er, r1ts, r1tr, r2s, r2r, moe_a, hid,
    sx_s, sx_r, sz_s, sz_r, tot_s, tot_r, h_in, h_b,
    sib_s, sib_r, own_p, m1_r, m2_s, m2_r,
    wsem, agss, agrs, sbss, sbrs, lsem,
    p1ss, p1rs, p2ss, p2rs, r1ss, r1rs, r1tss, r1trs, r2ss, r2rs,
    sxss, sxrs, szss, szrs, ttss, ttrs, rsss, rsrs, m1ss, m1rs, m2ss, m2rs,
):
    n_ep, zn, xnn, tok, d, ff = dims
    slots = n_ep * 8
    ep = lax.axis_index("ep")
    tp = lax.axis_index("tp")
    y = tp // 2
    core = tp % 2
    sib = y * 2 + (1 - core)

    def at_y(k):
        return lax.rem(y + k, 4) * 2

    right, left = at_y(1) + core, at_y(3) + core
    order = [(0, 1), (1, 0), (0, 3), (3, 0), (1, 1), (3, 3), (1, 3), (3, 1),
             (2, 0), (0, 2), (1, 2), (3, 2), (2, 1), (2, 3), (2, 2)]
    order = [(a, b) for a, b in order if a < zn and b < xnn]
    n_off = len(order)
    eps = [
        lax.rem(ep // xnn + a, zn) * xnn + lax.rem(ep % xnn + b, xnn) for a, b in order
    ]
    tps = [at_y(a) + lax.rem(core + b, 2)
           for a, b in ((1, 0), (3, 1), (1, 1), (3, 0), (2, 0), (2, 1), (0, 1))]

    def load(n, src, dst):
        return pltpu.make_async_copy(src, dst, wsem.at[n])

    first = [
        load(8, x_ref.at[pl.ds(0, 64)], x_v.at[pl.ds(0, 64)]),
        load(9, mgain_in, mgain_ref),
        load(10, x_ref.at[pl.ds(64, 64)], x_v.at[pl.ds(64, 64)]),
        load(11, e_ref, e_v),
        load(12, egain_in, egain_ref),
        load(13, routes_in, routes_ref),
        load(14, ld_in, ld_ref),
        load(15, rot_t_ref, rot_v),
        load(16, rot_b_in.at[ep], rot_b_ref),
        load(17, hgain_in, hgain_ref),
        load(18, gw_in, gw_ref),
        load(19, pw_in, pw_ref),
    ]
    loads = [
        pltpu.make_async_copy(wq_ref, w_in.at[:, pl.ds(0, KD)], wsem.at[0]),
        pltpu.make_async_copy(wk_ref, w_in.at[:, pl.ds(KD, KD)], wsem.at[1]),
        pltpu.make_async_copy(wv_ref, w_in.at[:, pl.ds(2 * KD, VD)], wsem.at[2]),
        pltpu.make_async_copy(wg_ref, w_in.at[:, pl.ds(2 * KD + VD, VD)], wsem.at[3]),
        pltpu.make_async_copy(wo_ref, w_out, wsem.at[4]),
        pltpu.make_async_copy(eg_ref, w_eg, wsem.at[5]),
        pltpu.make_async_copy(eu_ref, w_eu, wsem.at[6]),
        pltpu.make_async_copy(ed_ref, w_ed, wsem.at[7]),
    ]
    for c in first[:3]:
        c.start()

    barrier = pltpu.get_barrier_semaphore()
    for t in tps:
        pl.semaphore_signal(barrier, inc=1, device_id={"tp": t}, device_id_type=MESH)
    for t in eps:
        pl.semaphore_signal(barrier, inc=1, device_id={"ep": t}, device_id_type=MESH)
    for c in first[3:] + loads:
        c.start()

    for c in first[:2]:
        c.wait()
    norm_rows(x_v, mgain_ref, xn.at[tp], 0, 64, 32)
    first[2].wait()
    norm_rows(x_v, mgain_ref, xn.at[tp], 64, 64, 32)
    pl.semaphore_wait(barrier, n_off + 7)

    def rcopy(src, dst, ss, rs, who):
        return pltpu.make_async_remote_copy(
            src_ref=src, dst_ref=dst, send_sem=ss, recv_sem=rs,
            device_id=who, device_id_type=MESH,
        )

    def ag(direction, piece):
        half = pl.ds(64 * ((piece + direction) % 2), 64)
        if piece == 2:
            half = pl.ds(64 * direction, 64)
            block = left if direction == 0 else right
        else:
            block = tp
        ref = xn.at[block, half]
        return rcopy(ref, ref, agss.at[direction, piece], agrs.at[direction, piece],
                     {"tp": right if direction == 0 else left})

    def ag_in(direction, piece):
        half = pl.ds(64 * ((piece + direction) % 2), 64)
        if piece == 2:
            half = pl.ds(64 * direction, 64)
            block = at_y(2) + core
        else:
            block = left if direction == 0 else right
        ref = xn.at[block, half]
        return rcopy(ref, ref, agss.at[direction, piece], agrs.at[direction, piece],
                     {"tp": right if direction == 0 else left})

    def sb_half(half, mine=True):
        block = at_y(2) + (core if mine else 1 - core)
        ref = xn.at[block, pl.ds(64 * half, 64)]
        return rcopy(ref, ref, sbss.at[2 + 2 * half], sbrs.at[2 + 2 * half], {"tp": sib})

    def sb(k, mine=True):
        block = at_y(k) + (core if mine else 1 - core)
        ref = xn.at[block]
        return rcopy(ref, ref, sbss.at[k], sbrs.at[k], {"tp": sib})

    for piece in range(2):
        for direction in range(2):
            ag(direction, piece).start()
    sb(0).start()

    for c in first[3:6]:
        c.wait()
    norm_rows(e_v, egain_ref, xe, 0, tok, min(tok, 32))
    e_of = lax.broadcasted_iota(jnp.int32, (slots, tok), 0)
    hit0 = e_of == routes_ref[0:1, :]
    hit1 = e_of == routes_ref[1:2, :]
    hits = jnp.where(jnp.logical_or(hit0, hit1), 1.0, 0.0)
    before = lax.broadcasted_iota(jnp.int32, (tok, tok), 0) < lax.broadcasted_iota(
        jnp.int32, (tok, tok), 1
    )
    rank = dot(hits.astype(BF16), jnp.where(before, 1.0, 0.0).astype(BF16))

    def ep_send(buf, into, f, ss, rs):
        for t in eps:
            rcopy(buf.at[f, t], into.at[f, ep], ss.at[f], rs.at[f], {"ep": t}).start()
        pltpu.make_async_copy(buf.at[f, ep], into.at[f, ep], lsem).start()
        pltpu.make_async_copy(buf.at[f, ep], into.at[f, ep], lsem).wait()

    def tp_send(buf, into, f, ss, rs):
        for t in tps:
            rcopy(buf.at[f, t], into.at[f, tp], ss.at[f], rs.at[f], {"tp": t}).start()
        pltpu.make_async_copy(buf.at[f, tp], into.at[f, tp], lsem).start()
        pltpu.make_async_copy(buf.at[f, tp], into.at[f, tp], lsem).wait()

    def all_of(buf, f, n, sem):
        ref = buf.at[f, pl.ds(0, n)]
        return pltpu.make_async_copy(ref, ref, sem.at[f])

    for k in range(CAP):
        here = jnp.abs(rank - float(k)) < 0.5
        s0 = jnp.where(jnp.logical_and(hit0, here), 1.0, 0.0)
        s1 = jnp.where(jnp.logical_and(hit1, here), 1.0, 0.0)
        sel[k, 0] = s0.astype(BF16)
        sel[k, 1] = s1.astype(BF16)
        part = dot((s0 + s1).astype(BF16), xe[...])
        p1s[k] = part.reshape(n_ep, 8, d).astype(BF16)
        ep_send(p1s, p1r, k, p1ss, p1rs)

    for c in first[6:]:
        c.wait()
    upto = lax.broadcasted_iota(jnp.int32, (128, 128), 0) <= lax.broadcasted_iota(
        jnp.int32, (128, 128), 1
    )
    inside = dot(ld_ref[...], jnp.where(upto, 1.0, 0.0), precision=HI)
    run = jnp.zeros((1, 1), F32)
    for b in range(8):
        row = inside[b:b + 1, :] + run
        c_row[b:b + 1, :] = row
        c_col[b] = jnp.transpose(jnp.broadcast_to(row, (128, 128)))
        run = run + inside[b:b + 1, 127:128]
    tot_s[...] = jnp.broadcast_to(run, (8, 128))

    def tt_copy(o):
        return rcopy(tot_s, tot_r.at[ep], ttss.at[o], ttrs.at[o], {"ep": eps[o]})

    def sx_copy(b):
        x_me = ep % xnn
        return rcopy(sx_s, sx_r.at[x_me], sxss.at[b], sxrs.at[b],
                     {"ep": ep - x_me + lax.rem(x_me + b, xnn)})

    def sz_copy(a):
        return rcopy(sz_s, sz_r.at[ep // xnn], szss.at[a], szrs.at[a],
                     {"ep": lax.rem(ep // xnn + a, zn) * xnn + ep % xnn})

    for o in range(n_off):
        tt_copy(o).start()
    tot_r[ep] = tot_s[...]

    turn = rot_b_ref[...]
    cb = turn[:, :KD]
    sbn = turn[:, KD:]
    for i in range(4):
        at = pl.ds(i * 256, 256)
        ct = rot_v[at, :KD]
        st = rot_v[at, KD:]
        rot_c[at, :] = ct * cb - st * sbn
        rot_s[at, :] = st * cb + ct * sbn

    pm_r = lax.broadcasted_iota(jnp.int32, (slots, slots), 0)
    pm_c = lax.broadcasted_iota(jnp.int32, (slots, slots), 1)
    perm[...] = jnp.where(
        pm_r == (pm_c & 7) * n_ep + (pm_c >> 3), 1.0, 0.0
    ).astype(BF16)

    for k in range(1, CAP):
        for j in range(2):
            sel[k, j] = dot(perm[...], sel[k, j]).astype(BF16)

    def relay(f, got, got_sem, buf, into, ss, rs):
        all_of(got, f, n_off, got_sem).wait()
        moved = dot(perm[...], rows_of(got[f])).astype(BF16)
        buf[f] = moved.reshape(8, n_ep, d)
        tp_send(buf, into, f, ss, rs)

    def forward(f):
        relay(f, p1r, p1rs, p2s, p2r, p2ss, p2rs)

    def project(first, count):
        rows = pl.ds(pl.multiple_of(first * 128, 128), count * 128)
        xb = xn[pl.ds(first, count)].reshape(count * 128, d)
        cos = rot_c[rows, :]
        sin = rot_s[rows, :]
        qk = dot(xb, w_in[:, :2 * KD])
        for i, ref in enumerate((rq, rk)):
            part = qk[:, i * KD:(i + 1) * KD].astype(BF16).astype(F32)
            ref[rows, :] = (part * cos + pltpu.roll(part, KD // 2, 1) * sin).astype(BF16)
        vv[rows, :] = dot(xb, w_in[:, 2 * KD:2 * KD + VD]).astype(BF16)
        gg[rows, :] = dot(xb, w_in[:, 2 * KD + VD:]).astype(BF16)

    def state_of(part):
        total = jnp.zeros((KD, VD), F32)
        for k in ((0,), (1, 3), (2,))[part]:
            first = at_y(k)
            at = pl.ds(pl.multiple_of(first * 128, 256), 256)
            left_over = jnp.exp(run - c_col[pl.ds(first, 2)].reshape(256, 128))
            kw = (rk[at, :].astype(F32) * left_over).astype(BF16)
            total = total + dot_t0(kw, vv[at, :])
        return total

    for c in loads[:4]:
        c.wait()
    sb(0, False).wait_recv()
    project(at_y(0), 2)
    for direction in range(2):
        ag_in(direction, 0).wait_recv()
        ag(direction, 2).start()
    forward(0)
    for direction in range(2):
        ag_in(direction, 1).wait_recv()
    sb(3).start()
    sb(1).start()
    forward(1)
    sb(3, False).wait_recv()
    project(at_y(3), 2)
    sb(1, False).wait_recv()
    project(at_y(1), 2)
    for direction in range(2):
        ag_in(direction, 2).wait_recv()
        sb_half(direction).start()
    state = state_of(0) + state_of(1)
    project(at_y(2) + core, 1)
    for direction in range(2):
        sb_half(direction, False).wait_recv()
    project(at_y(2) + 1 - core, 1)

    state = state + state_of(2)
    sx_s[...] = state.astype(BF16)
    sx_r[ep % xnn] = state.astype(BF16)

    causal = lax.broadcasted_iota(jnp.int32, (256, 256), 0) >= lax.broadcasted_iota(
        jnp.int32, (256, 256), 1
    )
    for b in range(1, xnn):
        sx_copy(b).start()
    forward(2)

    for i in range(4):
        qi = rq[pl.ds(i * 256, 256), :]
        ci = jnp.concatenate([c_col[2 * i], c_col[2 * i + 1]], axis=0)
        ci = jnp.concatenate([ci, ci], axis=1)
        out = jnp.zeros((256, VD), F32)
        for j in range(i + 1):
            at = pl.ds(j * 256, 256)
            cj = jnp.concatenate([c_row[2 * j:2 * j + 1, :], c_row[2 * j + 1:2 * j + 2, :]], axis=1)
            w = jnp.exp(jnp.minimum(ci - cj, 0.0))
            if i == j:
                w = jnp.where(causal, w, 0.0)
            dec = (dot_t1(qi, rk[at, :]) * w).astype(BF16)
            out = out + dot(dec, vv[at, :])
        lo[pl.ds(i * 256, 256), :] = out

    def expert_in(k):
        all_of(p2r, k, 7, p2rs).wait()
        xk = p2r[k].reshape(slots, d)

        @pl.loop(0, ff // 256)
        def _(n):
            at = pl.ds(pl.multiple_of(n * 256, 256), 256)
            g = dot(xk, w_eg[:, at])
            u = dot(xk, w_eu[:, at])
            hid[:, at] = (g / (1.0 + jnp.exp(-g)) * u).astype(BF16)

    def expert_out(k, along_tp):
        h = hid[...] if along_tp else dot_t0(perm[...], hid[...]).astype(BF16)
        for n in range(4):
            at = pl.ds(n * (d // 4), d // 4)
            part = dot(h, w_ed[:, n * (d // 4):(n + 1) * (d // 4)])
            if along_tp:
                r1ts[0, :, :, at] = part.astype(BF16).reshape(8, n_ep, d // 4)
            else:
                r1e[k, :, :, at] = part.reshape(n_ep, 8, d // 4).astype(BF16)

    for c in loads[4:]:
        c.wait()
    expert_in(0)

    def lanes(v):
        return jnp.concatenate([v, v], axis=1)

    for o in range(n_off):
        tt_copy(o).wait_recv()
    for b in range(1, xnn):
        sx_copy(b).wait_recv()
    zero = jnp.zeros((1, 128), F32)
    z_me, x_me = ep // xnn, ep % xnn
    row = z_me * xnn
    row_state = jnp.zeros((KD, VD), F32)
    my_state = jnp.zeros((KD, VD), F32)
    row_log, my_log = zero, zero
    for i in reversed(range(xnn)):
        t = tot_r[row + i, 0:1, :]
        part = sx_r[i].astype(F32)
        row_state = row_state + part * lanes(jnp.exp(row_log))
        row_log = row_log + t
        my_state = my_state + jnp.where(i < x_me, part * lanes(jnp.exp(my_log)), 0.0)
        my_log = my_log + jnp.where(i < x_me, t, 0.0)
    sz_s[...] = row_state.astype(BF16)
    sz_r[z_me] = jnp.zeros((KD, VD), BF16)
    h_in[...] = my_state
    for a in range(1, zn):
        sz_copy(a).start()
    expert_out(0, True)
    tp_send(r1ts, r1tr, 0, r1tss, r1trs)
    expert_in(1)
    expert_out(1, False)
    ep_send(r1e, r1er, 1, r1ss, r1rs)
    for a in range(1, zn):
        sz_copy(a).wait_recv()
    before_rows = jnp.zeros((KD, VD), F32)
    z_log = zero
    for i in reversed(range(zn)):
        t = zero
        for j in range(xnn):
            t = t + tot_r[i * xnn + j, 0:1, :]
        part = sz_r[i].astype(F32) * lanes(jnp.exp(z_log))
        before_rows = before_rows + jnp.where(i < z_me, part, 0.0)
        z_log = z_log + jnp.where(i < z_me, t, 0.0)
    h_b[...] = (h_in[...] + before_rows * lanes(jnp.exp(my_log))).astype(BF16)

    def partial_rows(block):
        at = pl.ds(pl.multiple_of(block * 128, 128), 128)
        col = jnp.exp(c_col[block])
        q = (rq[at, :].astype(F32) * col).astype(BF16)
        ret = lo[at, :] + dot(q, h_b[...])
        mean = jnp.mean(ret, axis=-1, keepdims=True)
        c = ret - mean
        var = jnp.mean(c * c, axis=-1, keepdims=True)
        normed = c * lax.rsqrt(var + EPSILON) * hgain_ref[...]
        g = gg[at, :].astype(F32)
        return (g / (1.0 + jnp.exp(-g)) * normed).astype(BF16)

    def relay_ep():
        all_of(r1tr, 0, 7, r1trs).wait()
        moved = dot_t0(perm[...], r1tr[0].reshape(slots, d))
        r1e[0] = moved.reshape(n_ep, 8, d).astype(BF16)
        ep_send(r1e, r1er, 0, r1ss, r1rs)

    def rs_sib(k):
        return rcopy(sib_s.at[k], sib_r.at[k], rsss.at[k], rsrs.at[k], {"tp": sib})

    def sib_part(k):
        gated = partial_rows(at_y(k) + 1 - core)
        sib_s[k] = dot(gated, w_out[...]).astype(BF16)

    def own_part(k):
        gated = partial_rows(at_y(k) + core)
        rs_sib(k).start()
        own_p[k] = dot(gated, w_out[...])

    def chip_sum(k):
        rs_sib(k).wait_recv()
        return own_p[k] + sib_r[k].astype(F32)

    def m1(direction):
        src = m2_s.at[2, pl.ds(64 * direction, 64)]
        return rcopy(src, m1_r.at[direction], m1ss.at[direction], m1rs.at[direction],
                     {"tp": right if direction == 0 else left})

    def m2(direction, half):
        src = m2_s.at[direction, pl.ds(64 * half, 64)]
        return rcopy(src, m2_r.at[direction, pl.ds(64 * half, 64)],
                     m2ss.at[direction, half], m2rs.at[direction, half],
                     {"tp": right if direction == 0 else left})

    sib_part(2)
    own_part(2)
    sib_part(1)
    m2_s[2] = chip_sum(2).astype(BF16)
    own_part(1)
    for direction in range(2):
        m1(direction).start()
    expert_in(2)
    expert_out(2, False)
    own_p[1] = chip_sum(1)
    m2_s[0, 64:128] = own_p[1, 64:128, :].astype(BF16)
    ep_send(r1e, r1er, 2, r1ss, r1rs)
    sib_part(3)
    own_part(3)
    m2(0, 1).start()
    relay_ep()
    own_p[3] = chip_sum(3)
    m2_s[1, 0:64] = own_p[3, 0:64, :].astype(BF16)
    relay(1, r1er, r1rs, r2s, r2r, r2ss, r2rs)
    m2(1, 0).start()
    sib_part(0)
    own_part(0)

    for direction in range(2):
        m1(direction).wait_recv()
        half = pl.ds(64 * direction, 64)
        m2_s[direction, half] = (
            own_p[1 if direction == 0 else 3, half, :] + m1_r[direction].astype(F32)
        ).astype(BF16)
    w0 = jnp.transpose(jnp.broadcast_to(gw_ref[...] * pw_ref[0:1, :], (128, tok)))
    w1 = jnp.transpose(jnp.broadcast_to(gw_ref[...] * pw_ref[1:2, :], (128, tok)))
    w0, w1 = w0[:, 0:1], w1[:, 0:1]
    for direction in range(2):
        m2(direction, direction).start()
    relay(2, r1er, r1rs, r2s, r2r, r2ss, r2rs)

    def combine(k, got):
        for n in range(4):
            at = pl.ds(n * (d // 4), d // 4)
            part = w0 * dot_t0(sel[k, 0], got[:, n * (d // 4):(n + 1) * (d // 4)])
            part = part + w1 * dot_t0(sel[k, 1], got[:, n * (d // 4):(n + 1) * (d // 4)])
            if k == 0:
                moe_a[:, at] = part
            elif k == 1:
                moe_a[:, at] += part
            else:
                moe_ref[:, at] = (moe_a[:, at] + part).astype(BF16)

    all_of(r1er, 0, n_off, r1rs).wait()
    combine(0, rows_of(r1er[0]))
    for direction in range(2):
        for half in range(2):
            m2(direction, half).wait_recv()
    mix_ref[...] = (
        chip_sum(0) + m2_r[0].astype(F32) + m2_r[1].astype(F32)
    ).astype(BF16)

    for k in range(1, CAP):
        all_of(r2r, k, 7, r2rs).wait()
        combine(k, r2r[k].reshape(slots, d))

    for direction in range(2):
        for piece in range(3):
            ag(direction, piece).wait_send()
        m1(direction).wait_send()
        for half in range(2):
            m2(direction, half).wait_send()
    for k in range(4):
        rs_sib(k).wait_send()
    for k in (0, 1, 3):
        sb(k).wait_send()
    for half in range(2):
        sb_half(half).wait_send()
    for k in range(CAP):
        all_of(p1s, k, n_off, p1ss).wait()
        all_of(p2s, k, 7, p2ss).wait()
        all_of(r1e, k, n_off, r1ss).wait()
        if k:
            all_of(r2s, k, 7, r2ss).wait()
    all_of(r1ts, 0, 7, r1tss).wait()
    for o in range(n_off):
        tt_copy(o).wait_send()
    for b in range(1, xnn):
        sx_copy(b).wait_send()
    for a in range(1, zn):
        sz_copy(a).wait_send()


def place(a_ref, b_ref, a_out, b_out, sem):
    outs = [
        pltpu.make_async_copy(a_ref, a_out, sem.at[0]),
        pltpu.make_async_copy(b_ref, b_out, sem.at[1]),
    ]
    for c in outs:
        c.start()
    for c in outs:
        c.wait()


def rotation_tables(n_ep, rows):
    half = KD // 2
    freq = (THETA ** (-np.arange(half) / half)).astype(np.float32).astype(np.float64)
    sign = np.concatenate([-np.ones(half), np.ones(half)])

    def both(positions):
        angles = np.tile(positions[:, None] * freq[None, :], (1, 2))
        return np.concatenate([np.cos(angles), np.sin(angles) * sign], axis=1)

    inner = both(np.arange(rows, dtype=np.float64))
    outer = both(rows * np.arange(n_ep, dtype=np.float64))
    return inner.astype(np.float32), outer.astype(np.float32)


def solution(mesh):
    n_ep = mesh.shape["ep"]
    zn, xnn = (4, 4) if n_ep == 16 else (n_ep, 1)

    def local(
        mixer_input, log_decay, mixer_gain, query_weight, key_weight, value_weight,
        gate_weight, head_gain, output_weight, expert_input, expert_gain, routes,
        group_weight, pair_weight, expert_gate, expert_up, expert_down,
    ):
        tok, d = expert_input.shape
        ff = expert_gate.shape[2]
        seg = log_decay.shape[0]
        slots = n_ep * 8
        rot_t, rot_b = rotation_tables(n_ep, seg)
        hbm = pl.BlockSpec(memory_space=pl.ANY)
        near = pl.BlockSpec(memory_space=pltpu.VMEM)
        in_specs = [hbm] * 19
        V = pltpu.VMEM
        DMA = pltpu.SemaphoreType.DMA
        scratch = [
            V((128, d), BF16), V((tok, d), BF16), V((seg, 2 * KD), F32),
            V((8, 128), F32), V((1, d), F32), V((1, VD), F32), V((1, d), F32),
            V((2, tok), jnp.int32), V((1, tok), F32), V((2, tok), F32), V((1, 2 * KD), F32),
            V((d, 2 * KD + 2 * VD), BF16), V((VD, d), BF16), V((d, ff), BF16),
            V((d, ff), BF16), V((ff, d), BF16),
            V((8, 128, d), BF16), V((tok, d), BF16), V((seg, KD), BF16), V((seg, KD), BF16),
            V((seg, VD), BF16), V((seg, VD), BF16), V((seg, VD), F32), V((seg, KD), F32),
            V((seg, KD), F32), V((8, 128, 128), F32), V((8, 128), F32),
            V((CAP, 2, slots, tok), BF16), V((slots, slots), BF16),
            V((CAP, n_ep, 8, d), BF16), V((CAP, n_ep, 8, d), BF16),
            V((CAP, 8, n_ep, d), BF16), V((CAP, 8, n_ep, d), BF16),
            V((CAP, n_ep, 8, d), BF16), V((CAP, n_ep, 8, d), BF16),
            V((1, 8, n_ep, d), BF16), V((1, 8, n_ep, d), BF16),
            V((CAP, 8, n_ep, d), BF16), V((CAP, 8, n_ep, d), BF16),
            V((tok, d), F32), V((slots, ff), BF16),
            V((KD, VD), BF16), V((xnn, KD, VD), BF16), V((KD, VD), BF16), V((zn, KD, VD), BF16),
            V((8, 128), F32), V((n_ep, 8, 128), F32), V((KD, VD), F32), V((KD, VD), BF16),
            V((4, 128, d), BF16), V((4, 128, d), BF16), V((4, 128, d), F32),
            V((2, 64, d), BF16), V((3, 128, d), BF16), V((2, 128, d), BF16),
            DMA((20,)), DMA((2, 3)), DMA((2, 3)), DMA((5,)), DMA((5,)), DMA,
            DMA((CAP,)), DMA((CAP,)), DMA((CAP,)), DMA((CAP,)), DMA((CAP,)), DMA((CAP,)),
            DMA((1,)), DMA((1,)), DMA((CAP,)), DMA((CAP,)),
            DMA((xnn,)), DMA((xnn,)), DMA((zn,)), DMA((zn,)), DMA((n_ep,)), DMA((n_ep,)),
            DMA((4,)), DMA((4,)), DMA((2,)), DMA((2,)), DMA((2, 2)), DMA((2, 2)),
        ]
        mixed, moe = pl.pallas_call(
            functools.partial(kernel, (n_ep, zn, xnn, tok, d, ff)),
            out_shape=(V(mixer_input.shape, BF16), V(expert_input.shape, BF16)),
            in_specs=in_specs,
            out_specs=(near, near),
            scratch_shapes=scratch,
            compiler_params=pltpu.CompilerParams(
                collective_id=0, has_side_effects=True, vmem_limit_bytes=58 * 2**20
            ),
        )(
            mixer_input, log_decay.reshape(8, 128), mixer_gain.reshape(1, -1),
            query_weight, key_weight, value_weight, gate_weight,
            head_gain.reshape(1, -1), output_weight, expert_input,
            expert_gain.reshape(1, -1), routes.T, group_weight.reshape(1, -1),
            pair_weight.T, expert_gate[0], expert_up[0], expert_down[0],
            jnp.asarray(rot_t), jnp.asarray(rot_b[:, None, :]),
        )
        return pl.pallas_call(
            place,
            out_shape=(
                jax.ShapeDtypeStruct(mixed.shape, BF16),
                jax.ShapeDtypeStruct(moe.shape, BF16),
            ),
            in_specs=[near, near],
            out_specs=(hbm, hbm),
            scratch_shapes=[DMA((2,))],
        )(*(pltpu.with_memory_space_constraint(v, pltpu.VMEM) for v in (mixed, moe)))

    return jax.shard_map(
        local,
        mesh=mesh,
        in_specs=(
            P(("ep", "tp"), None), P("ep", "tp"), P(), P(None, "tp"), P(None, "tp"),
            P(None, "tp"), P(None, "tp"), P("tp"), P("tp", None), P(("ep", "tp"), None),
            P(), P(("ep", "tp"), None), P(("ep", "tp")), P(("ep", "tp"), None),
            P(("ep", "tp"), None, None), P(("ep", "tp"), None, None),
            P(("ep", "tp"), None, None),
        ),
        out_specs=(P(("ep", "tp"), None), P(("ep", "tp"), None)),
        check_vma=False,
    )
```

```python
import functools

import jax
import jax.numpy as jnp
import numpy as np
from jax import lax
from jax.experimental import pallas as pl
from jax.experimental.pallas import tpu as pltpu
from jax.sharding import PartitionSpec as P

KD = 128
VD = 256
CAP = 3
EPSILON = 1e-05
THETA = 10000.0
MESH = pl.DeviceIdType.MESH
F32 = jnp.float32
BF16 = jnp.bfloat16
HI = lax.Precision.HIGHEST


def dot(a, b, **kw):
    return jnp.dot(a, b, preferred_element_type=F32, **kw)


def dot_t0(a, b):
    return lax.dot_general(a, b, (((0,), (0,)), ((), ())), preferred_element_type=F32)


def dot_t1(a, b):
    return lax.dot_general(a, b, (((1,), (1,)), ((), ())), preferred_element_type=F32)


def norm_rows(src, gain, dst, start, rows, step):
    @pl.loop(0, rows // step)
    def _(i):
        at = pl.ds(pl.multiple_of(start + i * step, step), step)
        m = src[at, :].astype(F32)
        mean = jnp.mean(m, axis=-1, keepdims=True)
        c = m - mean
        var = jnp.mean(c * c, axis=-1, keepdims=True)
        dst[at, :] = (c * lax.rsqrt(var + EPSILON) * gain[...]).astype(BF16)


def rows_of(x3):
    a, b, c = x3.shape
    return x3.astype(F32).reshape(a * b, c).astype(BF16)


def kernel(
    dims,
    x_ref, ld_in, mgain_in, wq_ref, wk_ref, wv_ref, wg_ref, hgain_in, wo_ref,
    e_ref, egain_in, routes_in, gw_in, pw_in, eg_ref, eu_ref, ed_ref,
    rot_t_ref, rot_b_in,
    mix_ref, moe_ref,
    x_v, e_v, rot_v,
    ld_ref, mgain_ref, hgain_ref, egain_ref, routes_ref, gw_ref, pw_ref, rot_b_ref,
    w_in, w_out, w_eg, w_eu, w_ed,
    xn, xe, rq, rk, vv, gg, lo, rot_c, rot_s, c_col, c_row,
    sel, perm,
    p1s, p1r, p2s, p2r, r1e, r1er, r1ts, r1tr, r2s, r2r, moe_a, hid,
    sx_s, sx_r, sz_s, sz_r, tot_s, tot_r, h_in, h_b,
    sib_s, sib_r, own_p, m1_r, m2_s, m2_r,
    wsem, agss, agrs, sbss, sbrs, lsem,
    p1ss, p1rs, p2ss, p2rs, r1ss, r1rs, r1tss, r1trs, r2ss, r2rs,
    sxss, sxrs, szss, szrs, ttss, ttrs, rsss, rsrs, m1ss, m1rs, m2ss, m2rs,
):
    n_ep, zn, xnn, tok, d, ff = dims
    slots = n_ep * 8
    ep = lax.axis_index("ep")
    tp = lax.axis_index("tp")
    y = tp // 2
    core = tp % 2
    sib = y * 2 + (1 - core)

    def at_y(k):
        return lax.rem(y + k, 4) * 2

    right, left = at_y(1) + core, at_y(3) + core
    order = [(0, 1), (1, 0), (0, 3), (3, 0), (1, 1), (3, 3), (1, 3), (3, 1),
             (2, 0), (0, 2), (1, 2), (3, 2), (2, 1), (2, 3), (2, 2)]
    order = [(a, b) for a, b in order if a < zn and b < xnn]
    n_off = len(order)
    eps = [
        lax.rem(ep // xnn + a, zn) * xnn + lax.rem(ep % xnn + b, xnn) for a, b in order
    ]
    tps = [at_y(a) + lax.rem(core + b, 2)
           for a, b in ((1, 0), (3, 1), (1, 1), (3, 0), (2, 0), (2, 1), (0, 1))]

    def load(n, src, dst):
        return pltpu.make_async_copy(src, dst, wsem.at[n])

    first = [
        load(8, x_ref.at[pl.ds(0, 64)], x_v.at[pl.ds(0, 64)]),
        load(9, mgain_in, mgain_ref),
        load(10, x_ref.at[pl.ds(64, 64)], x_v.at[pl.ds(64, 64)]),
        load(11, e_ref, e_v),
        load(12, egain_in, egain_ref),
        load(13, routes_in, routes_ref),
        load(14, ld_in, ld_ref),
        load(15, rot_t_ref, rot_v),
        load(16, rot_b_in.at[ep], rot_b_ref),
        load(17, hgain_in, hgain_ref),
        load(18, gw_in, gw_ref),
        load(19, pw_in, pw_ref),
    ]
    loads = [
        pltpu.make_async_copy(wq_ref, w_in.at[:, pl.ds(0, KD)], wsem.at[0]),
        pltpu.make_async_copy(wk_ref, w_in.at[:, pl.ds(KD, KD)], wsem.at[1]),
        pltpu.make_async_copy(wv_ref, w_in.at[:, pl.ds(2 * KD, VD)], wsem.at[2]),
        pltpu.make_async_copy(wg_ref, w_in.at[:, pl.ds(2 * KD + VD, VD)], wsem.at[3]),
        pltpu.make_async_copy(wo_ref, w_out, wsem.at[4]),
        pltpu.make_async_copy(eg_ref, w_eg, wsem.at[5]),
        pltpu.make_async_copy(eu_ref, w_eu, wsem.at[6]),
        pltpu.make_async_copy(ed_ref, w_ed, wsem.at[7]),
    ]
    for c in first[:3]:
        c.start()

    barrier = pltpu.get_barrier_semaphore()
    for t in tps:
        pl.semaphore_signal(barrier, inc=1, device_id={"tp": t}, device_id_type=MESH)
    for t in eps:
        pl.semaphore_signal(barrier, inc=1, device_id={"ep": t}, device_id_type=MESH)
    for c in first[3:] + loads:
        c.start()

    for c in first[:2]:
        c.wait()
    norm_rows(x_v, mgain_ref, xn.at[tp], 0, 64, 64)
    first[2].wait()
    norm_rows(x_v, mgain_ref, xn.at[tp], 64, 64, 64)
    pl.semaphore_wait(barrier, n_off + 7)

    def rcopy(src, dst, ss, rs, who):
        return pltpu.make_async_remote_copy(
            src_ref=src, dst_ref=dst, send_sem=ss, recv_sem=rs,
            device_id=who, device_id_type=MESH,
        )

    def ag(direction, piece):
        half = pl.ds(64 * ((piece + direction) % 2), 64)
        if piece == 2:
            half = pl.ds(64 * direction, 64)
            block = left if direction == 0 else right
        else:
            block = tp
        ref = xn.at[block, half]
        return rcopy(ref, ref, agss.at[direction, piece], agrs.at[direction, piece],
                     {"tp": right if direction == 0 else left})

    def ag_in(direction, piece):
        half = pl.ds(64 * ((piece + direction) % 2), 64)
        if piece == 2:
            half = pl.ds(64 * direction, 64)
            block = at_y(2) + core
        else:
            block = left if direction == 0 else right
        ref = xn.at[block, half]
        return rcopy(ref, ref, agss.at[direction, piece], agrs.at[direction, piece],
                     {"tp": right if direction == 0 else left})

    def sb_half(half, mine=True):
        block = at_y(2) + (core if mine else 1 - core)
        ref = xn.at[block, pl.ds(64 * half, 64)]
        return rcopy(ref, ref, sbss.at[2 + 2 * half], sbrs.at[2 + 2 * half], {"tp": sib})

    def sb(k, mine=True):
        block = at_y(k) + (core if mine else 1 - core)
        ref = xn.at[block]
        return rcopy(ref, ref, sbss.at[k], sbrs.at[k], {"tp": sib})

    for piece in range(2):
        for direction in range(2):
            ag(direction, piece).start()
    sb(0).start()

    for c in first[3:6]:
        c.wait()
    norm_rows(e_v, egain_ref, xe, 0, tok, min(tok, 64))
    e_of = lax.broadcasted_iota(jnp.int32, (slots, tok), 0)
    hit0 = e_of == routes_ref[0:1, :]
    hit1 = e_of == routes_ref[1:2, :]
    hits = jnp.where(jnp.logical_or(hit0, hit1), 1.0, 0.0)
    before = lax.broadcasted_iota(jnp.int32, (tok, tok), 0) < lax.broadcasted_iota(
        jnp.int32, (tok, tok), 1
    )
    rank = dot(hits.astype(BF16), jnp.where(before, 1.0, 0.0).astype(BF16))

    def ep_send(buf, into, f, ss, rs):
        for t in eps:
            rcopy(buf.at[f, t], into.at[f, ep], ss.at[f], rs.at[f], {"ep": t}).start()
        pltpu.make_async_copy(buf.at[f, ep], into.at[f, ep], lsem).start()
        pltpu.make_async_copy(buf.at[f, ep], into.at[f, ep], lsem).wait()

    def tp_send(buf, into, f, ss, rs):
        for t in tps:
            rcopy(buf.at[f, t], into.at[f, tp], ss.at[f], rs.at[f], {"tp": t}).start()
        pltpu.make_async_copy(buf.at[f, tp], into.at[f, tp], lsem).start()
        pltpu.make_async_copy(buf.at[f, tp], into.at[f, tp], lsem).wait()

    def all_of(buf, f, n, sem):
        ref = buf.at[f, pl.ds(0, n)]
        return pltpu.make_async_copy(ref, ref, sem.at[f])

    for k in range(CAP):
        here = jnp.abs(rank - float(k)) < 0.5
        s0 = jnp.where(jnp.logical_and(hit0, here), 1.0, 0.0)
        s1 = jnp.where(jnp.logical_and(hit1, here), 1.0, 0.0)
        sel[k, 0] = s0.astype(BF16)
        sel[k, 1] = s1.astype(BF16)
        part = dot((s0 + s1).astype(BF16), xe[...])
        p1s[k] = part.reshape(n_ep, 8, d).astype(BF16)
        ep_send(p1s, p1r, k, p1ss, p1rs)

    for c in first[6:]:
        c.wait()
    upto = lax.broadcasted_iota(jnp.int32, (128, 128), 0) <= lax.broadcasted_iota(
        jnp.int32, (128, 128), 1
    )
    inside = dot(ld_ref[...], jnp.where(upto, 1.0, 0.0), precision=HI)
    run = jnp.zeros((1, 1), F32)
    for b in range(8):
        row = inside[b:b + 1, :] + run
        c_row[b:b + 1, :] = row
        c_col[b] = jnp.transpose(jnp.broadcast_to(row, (128, 128)))
        run = run + inside[b:b + 1, 127:128]
    tot_s[...] = jnp.broadcast_to(run, (8, 128))

    def tt_copy(o):
        return rcopy(tot_s, tot_r.at[ep], ttss.at[o], ttrs.at[o], {"ep": eps[o]})

    def sx_copy(b):
        x_me = ep % xnn
        return rcopy(sx_s, sx_r.at[x_me], sxss.at[b], sxrs.at[b],
                     {"ep": ep - x_me + lax.rem(x_me + b, xnn)})

    def sz_copy(a):
        return rcopy(sz_s, sz_r.at[ep // xnn], szss.at[a], szrs.at[a],
                     {"ep": lax.rem(ep // xnn + a, zn) * xnn + ep % xnn})

    for o in range(n_off):
        tt_copy(o).start()
    tot_r[ep] = tot_s[...]

    turn = rot_b_ref[...]
    cb = turn[:, :KD]
    sbn = turn[:, KD:]
    for i in range(4):
        at = pl.ds(i * 256, 256)
        ct = rot_v[at, :KD]
        st = rot_v[at, KD:]
        rot_c[at, :] = ct * cb - st * sbn
        rot_s[at, :] = st * cb + ct * sbn

    pm_r = lax.broadcasted_iota(jnp.int32, (slots, slots), 0)
    pm_c = lax.broadcasted_iota(jnp.int32, (slots, slots), 1)
    perm[...] = jnp.where(
        pm_r == (pm_c & 7) * n_ep + (pm_c >> 3), 1.0, 0.0
    ).astype(BF16)

    for k in range(1, CAP):
        for j in range(2):
            sel[k, j] = dot(perm[...], sel[k, j]).astype(BF16)

    def relay(f, got, got_sem, buf, into, ss, rs):
        all_of(got, f, n_off, got_sem).wait()
        moved = dot(perm[...], rows_of(got[f])).astype(BF16)
        buf[f] = moved.reshape(8, n_ep, d)
        tp_send(buf, into, f, ss, rs)

    def forward(f):
        relay(f, p1r, p1rs, p2s, p2r, p2ss, p2rs)

    def project(first, count):
        rows = pl.ds(pl.multiple_of(first * 128, 128), count * 128)
        xb = xn[pl.ds(first, count)].reshape(count * 128, d)
        cos = rot_c[rows, :]
        sin = rot_s[rows, :]
        qk = dot(xb, w_in[:, :2 * KD])
        for i, ref in enumerate((rq, rk)):
            part = qk[:, i * KD:(i + 1) * KD].astype(BF16).astype(F32)
            ref[rows, :] = (part * cos + pltpu.roll(part, KD // 2, 1) * sin).astype(BF16)
        vv[rows, :] = dot(xb, w_in[:, 2 * KD:2 * KD + VD]).astype(BF16)
        gg[rows, :] = dot(xb, w_in[:, 2 * KD + VD:]).astype(BF16)

    def state_of(part):
        total = jnp.zeros((KD, VD), F32)
        for k in ((0,), (1, 3), (2,))[part]:
            first = at_y(k)
            at = pl.ds(pl.multiple_of(first * 128, 256), 256)
            left_over = jnp.exp(run - c_col[pl.ds(first, 2)].reshape(256, 128))
            kw = (rk[at, :].astype(F32) * left_over).astype(BF16)
            total = total + dot_t0(kw, vv[at, :])
        return total

    for c in loads[:4]:
        c.wait()
    sb(0, False).wait_recv()
    project(at_y(0), 2)
    for direction in range(2):
        ag_in(direction, 0).wait_recv()
        ag(direction, 2).start()
    forward(0)
    for direction in range(2):
        ag_in(direction, 1).wait_recv()
    sb(3).start()
    sb(1).start()
    forward(1)
    sb(3, False).wait_recv()
    project(at_y(3), 2)
    sb(1, False).wait_recv()
    project(at_y(1), 2)
    for direction in range(2):
        ag_in(direction, 2).wait_recv()
        sb_half(direction).start()
    state = state_of(0) + state_of(1)
    project(at_y(2) + core, 1)
    for direction in range(2):
        sb_half(direction, False).wait_recv()
    project(at_y(2) + 1 - core, 1)

    state = state + state_of(2)
    sx_s[...] = state.astype(BF16)
    sx_r[ep % xnn] = state.astype(BF16)

    causal = lax.broadcasted_iota(jnp.int32, (256, 256), 0) >= lax.broadcasted_iota(
        jnp.int32, (256, 256), 1
    )
    for b in range(1, xnn):
        sx_copy(b).start()
    forward(2)

    for i in range(4):
        qi = rq[pl.ds(i * 256, 256), :]
        ci = jnp.concatenate([c_col[2 * i], c_col[2 * i + 1]], axis=0)
        ci = jnp.concatenate([ci, ci], axis=1)
        out = jnp.zeros((256, VD), F32)
        for j in range(i + 1):
            at = pl.ds(j * 256, 256)
            cj = jnp.concatenate([c_row[2 * j:2 * j + 1, :], c_row[2 * j + 1:2 * j + 2, :]], axis=1)
            w = jnp.exp(jnp.minimum(ci - cj, 0.0))
            if i == j:
                w = jnp.where(causal, w, 0.0)
            dec = (dot_t1(qi, rk[at, :]) * w).astype(BF16)
            out = out + dot(dec, vv[at, :])
        lo[pl.ds(i * 256, 256), :] = out

    def expert_in(k):
        all_of(p2r, k, 7, p2rs).wait()
        xk = p2r[k].reshape(slots, d)

        @pl.loop(0, ff // 256)
        def _(n):
            at = pl.ds(pl.multiple_of(n * 256, 256), 256)
            g = dot(xk, w_eg[:, at])
            u = dot(xk, w_eu[:, at])
            hid[:, at] = (g / (1.0 + jnp.exp(-g)) * u).astype(BF16)

    def expert_out(k, along_tp):
        h = hid[...] if along_tp else dot_t0(perm[...], hid[...]).astype(BF16)
        for n in range(4):
            at = pl.ds(n * (d // 4), d // 4)
            part = dot(h, w_ed[:, n * (d // 4):(n + 1) * (d // 4)])
            if along_tp:
                r1ts[0, :, :, at] = part.astype(BF16).reshape(8, n_ep, d // 4)
            else:
                r1e[k, :, :, at] = part.reshape(n_ep, 8, d // 4).astype(BF16)

    for c in loads[4:]:
        c.wait()
    expert_in(0)

    def lanes(v):
        return jnp.concatenate([v, v], axis=1)

    for o in range(n_off):
        tt_copy(o).wait_recv()
    for b in range(1, xnn):
        sx_copy(b).wait_recv()
    zero = jnp.zeros((1, 128), F32)
    z_me, x_me = ep // xnn, ep % xnn
    row = z_me * xnn
    row_state = jnp.zeros((KD, VD), F32)
    my_state = jnp.zeros((KD, VD), F32)
    row_log, my_log = zero, zero
    for i in reversed(range(xnn)):
        t = tot_r[row + i, 0:1, :]
        part = sx_r[i].astype(F32)
        row_state = row_state + part * lanes(jnp.exp(row_log))
        row_log = row_log + t
        my_state = my_state + jnp.where(i < x_me, part * lanes(jnp.exp(my_log)), 0.0)
        my_log = my_log + jnp.where(i < x_me, t, 0.0)
    sz_s[...] = row_state.astype(BF16)
    sz_r[z_me] = jnp.zeros((KD, VD), BF16)
    h_in[...] = my_state
    for a in range(1, zn):
        sz_copy(a).start()
    expert_out(0, True)
    tp_send(r1ts, r1tr, 0, r1tss, r1trs)
    expert_in(1)
    expert_out(1, False)
    ep_send(r1e, r1er, 1, r1ss, r1rs)
    for a in range(1, zn):
        sz_copy(a).wait_recv()
    before_rows = jnp.zeros((KD, VD), F32)
    z_log = zero
    for i in reversed(range(zn)):
        t = zero
        for j in range(xnn):
            t = t + tot_r[i * xnn + j, 0:1, :]
        part = sz_r[i].astype(F32) * lanes(jnp.exp(z_log))
        before_rows = before_rows + jnp.where(i < z_me, part, 0.0)
        z_log = z_log + jnp.where(i < z_me, t, 0.0)
    h_b[...] = (h_in[...] + before_rows * lanes(jnp.exp(my_log))).astype(BF16)

    def partial_rows(block):
        at = pl.ds(pl.multiple_of(block * 128, 128), 128)
        col = jnp.exp(c_col[block])
        q = (rq[at, :].astype(F32) * col).astype(BF16)
        ret = lo[at, :] + dot(q, h_b[...])
        mean = jnp.mean(ret, axis=-1, keepdims=True)
        c = ret - mean
        var = jnp.mean(c * c, axis=-1, keepdims=True)
        normed = c * lax.rsqrt(var + EPSILON) * hgain_ref[...]
        g = gg[at, :].astype(F32)
        return (g / (1.0 + jnp.exp(-g)) * normed).astype(BF16)

    def relay_ep():
        all_of(r1tr, 0, 7, r1trs).wait()
        moved = dot_t0(perm[...], r1tr[0].reshape(slots, d))
        r1e[0] = moved.reshape(n_ep, 8, d).astype(BF16)
        ep_send(r1e, r1er, 0, r1ss, r1rs)

    def rs_sib(k):
        return rcopy(sib_s.at[k], sib_r.at[k], rsss.at[k], rsrs.at[k], {"tp": sib})

    def sib_part(k):
        gated = partial_rows(at_y(k) + 1 - core)
        sib_s[k] = dot(gated, w_out[...]).astype(BF16)

    def own_part(k):
        gated = partial_rows(at_y(k) + core)
        rs_sib(k).start()
        own_p[k] = dot(gated, w_out[...])

    def chip_sum(k):
        rs_sib(k).wait_recv()
        return own_p[k] + sib_r[k].astype(F32)

    def m1(direction):
        src = m2_s.at[2, pl.ds(64 * direction, 64)]
        return rcopy(src, m1_r.at[direction], m1ss.at[direction], m1rs.at[direction],
                     {"tp": right if direction == 0 else left})

    def m2(direction, half):
        src = m2_s.at[direction, pl.ds(64 * half, 64)]
        return rcopy(src, m2_r.at[direction, pl.ds(64 * half, 64)],
                     m2ss.at[direction, half], m2rs.at[direction, half],
                     {"tp": right if direction == 0 else left})

    sib_part(2)
    own_part(2)
    sib_part(1)
    m2_s[2] = chip_sum(2).astype(BF16)
    own_part(1)
    for direction in range(2):
        m1(direction).start()
    expert_in(2)
    expert_out(2, False)
    own_p[1] = chip_sum(1)
    m2_s[0, 64:128] = own_p[1, 64:128, :].astype(BF16)
    ep_send(r1e, r1er, 2, r1ss, r1rs)
    sib_part(3)
    own_part(3)
    m2(0, 1).start()
    relay_ep()
    own_p[3] = chip_sum(3)
    m2_s[1, 0:64] = own_p[3, 0:64, :].astype(BF16)
    relay(1, r1er, r1rs, r2s, r2r, r2ss, r2rs)
    m2(1, 0).start()
    sib_part(0)
    own_part(0)

    for direction in range(2):
        m1(direction).wait_recv()
        half = pl.ds(64 * direction, 64)
        m2_s[direction, half] = (
            own_p[1 if direction == 0 else 3, half, :] + m1_r[direction].astype(F32)
        ).astype(BF16)
    w0 = jnp.transpose(jnp.broadcast_to(gw_ref[...] * pw_ref[0:1, :], (128, tok)))
    w1 = jnp.transpose(jnp.broadcast_to(gw_ref[...] * pw_ref[1:2, :], (128, tok)))
    w0, w1 = w0[:, 0:1], w1[:, 0:1]
    for direction in range(2):
        m2(direction, direction).start()
    relay(2, r1er, r1rs, r2s, r2r, r2ss, r2rs)

    def combine(k, got):
        for n in range(4):
            at = pl.ds(n * (d // 4), d // 4)
            part = w0 * dot_t0(sel[k, 0], got[:, n * (d // 4):(n + 1) * (d // 4)])
            part = part + w1 * dot_t0(sel[k, 1], got[:, n * (d // 4):(n + 1) * (d // 4)])
            if k == 0:
                moe_a[:, at] = part
            elif k == 1:
                moe_a[:, at] += part
            else:
                moe_ref[:, at] = (moe_a[:, at] + part).astype(BF16)

    all_of(r1er, 0, n_off, r1rs).wait()
    combine(0, rows_of(r1er[0]))

    all_of(r2r, 1, 7, r2rs).wait()
    combine(1, r2r[1].reshape(slots, d))
    for direction in range(2):
        for half in range(2):
            m2(direction, half).wait_recv()
    mix_ref[...] = (
        chip_sum(0) + m2_r[0].astype(F32) + m2_r[1].astype(F32)
    ).astype(BF16)
    all_of(r2r, 2, 7, r2rs).wait()
    combine(2, r2r[2].reshape(slots, d))

    for direction in range(2):
        for piece in range(3):
            ag(direction, piece).wait_send()
        m1(direction).wait_send()
        for half in range(2):
            m2(direction, half).wait_send()
    for k in range(4):
        rs_sib(k).wait_send()
    for k in (0, 1, 3):
        sb(k).wait_send()
    for half in range(2):
        sb_half(half).wait_send()
    for k in range(CAP):
        all_of(p1s, k, n_off, p1ss).wait()
        all_of(p2s, k, 7, p2ss).wait()
        all_of(r1e, k, n_off, r1ss).wait()
        if k:
            all_of(r2s, k, 7, r2ss).wait()
    all_of(r1ts, 0, 7, r1tss).wait()
    for o in range(n_off):
        tt_copy(o).wait_send()
    for b in range(1, xnn):
        sx_copy(b).wait_send()
    for a in range(1, zn):
        sz_copy(a).wait_send()


def place(a_ref, b_ref, a_out, b_out, sem):
    outs = [
        pltpu.make_async_copy(a_ref, a_out, sem.at[0]),
        pltpu.make_async_copy(b_ref, b_out, sem.at[1]),
    ]
    for c in outs:
        c.start()
    for c in outs:
        c.wait()


def rotation_tables(n_ep, rows):
    half = KD // 2
    freq = (THETA ** (-np.arange(half) / half)).astype(np.float32).astype(np.float64)
    sign = np.concatenate([-np.ones(half), np.ones(half)])

    def both(positions):
        angles = np.tile(positions[:, None] * freq[None, :], (1, 2))
        return np.concatenate([np.cos(angles), np.sin(angles) * sign], axis=1)

    inner = both(np.arange(rows, dtype=np.float64))
    outer = both(rows * np.arange(n_ep, dtype=np.float64))
    return inner.astype(np.float32), outer.astype(np.float32)


def solution(mesh):
    n_ep = mesh.shape["ep"]
    zn, xnn = (4, 4) if n_ep == 16 else (n_ep, 1)

    def local(
        mixer_input, log_decay, mixer_gain, query_weight, key_weight, value_weight,
        gate_weight, head_gain, output_weight, expert_input, expert_gain, routes,
        group_weight, pair_weight, expert_gate, expert_up, expert_down,
    ):
        tok, d = expert_input.shape
        ff = expert_gate.shape[2]
        seg = log_decay.shape[0]
        slots = n_ep * 8
        rot_t, rot_b = rotation_tables(n_ep, seg)
        hbm = pl.BlockSpec(memory_space=pl.ANY)
        near = pl.BlockSpec(memory_space=pltpu.VMEM)
        in_specs = [hbm] * 19
        V = pltpu.VMEM
        DMA = pltpu.SemaphoreType.DMA
        scratch = [
            V((128, d), BF16), V((tok, d), BF16), V((seg, 2 * KD), F32),
            V((8, 128), F32), V((1, d), F32), V((1, VD), F32), V((1, d), F32),
            V((2, tok), jnp.int32), V((1, tok), F32), V((2, tok), F32), V((1, 2 * KD), F32),
            V((d, 2 * KD + 2 * VD), BF16), V((VD, d), BF16), V((d, ff), BF16),
            V((d, ff), BF16), V((ff, d), BF16),
            V((8, 128, d), BF16), V((tok, d), BF16), V((seg, KD), BF16), V((seg, KD), BF16),
            V((seg, VD), BF16), V((seg, VD), BF16), V((seg, VD), F32), V((seg, KD), F32),
            V((seg, KD), F32), V((8, 128, 128), F32), V((8, 128), F32),
            V((CAP, 2, slots, tok), BF16), V((slots, slots), BF16),
            V((CAP, n_ep, 8, d), BF16), V((CAP, n_ep, 8, d), BF16),
            V((CAP, 8, n_ep, d), BF16), V((CAP, 8, n_ep, d), BF16),
            V((CAP, n_ep, 8, d), BF16), V((CAP, n_ep, 8, d), BF16),
            V((1, 8, n_ep, d), BF16), V((1, 8, n_ep, d), BF16),
            V((CAP, 8, n_ep, d), BF16), V((CAP, 8, n_ep, d), BF16),
            V((tok, d), F32), V((slots, ff), BF16),
            V((KD, VD), BF16), V((xnn, KD, VD), BF16), V((KD, VD), BF16), V((zn, KD, VD), BF16),
            V((8, 128), F32), V((n_ep, 8, 128), F32), V((KD, VD), F32), V((KD, VD), BF16),
            V((4, 128, d), BF16), V((4, 128, d), BF16), V((4, 128, d), F32),
            V((2, 64, d), BF16), V((3, 128, d), BF16), V((2, 128, d), BF16),
            DMA((20,)), DMA((2, 3)), DMA((2, 3)), DMA((5,)), DMA((5,)), DMA,
            DMA((CAP,)), DMA((CAP,)), DMA((CAP,)), DMA((CAP,)), DMA((CAP,)), DMA((CAP,)),
            DMA((1,)), DMA((1,)), DMA((CAP,)), DMA((CAP,)),
            DMA((xnn,)), DMA((xnn,)), DMA((zn,)), DMA((zn,)), DMA((n_ep,)), DMA((n_ep,)),
            DMA((4,)), DMA((4,)), DMA((2,)), DMA((2,)), DMA((2, 2)), DMA((2, 2)),
        ]
        mixed, moe = pl.pallas_call(
            functools.partial(kernel, (n_ep, zn, xnn, tok, d, ff)),
            out_shape=(V(mixer_input.shape, BF16), V(expert_input.shape, BF16)),
            in_specs=in_specs,
            out_specs=(near, near),
            scratch_shapes=scratch,
            compiler_params=pltpu.CompilerParams(
                collective_id=0, has_side_effects=True, vmem_limit_bytes=58 * 2**20
            ),
        )(
            mixer_input, log_decay.reshape(8, 128), mixer_gain.reshape(1, -1),
            query_weight, key_weight, value_weight, gate_weight,
            head_gain.reshape(1, -1), output_weight, expert_input,
            expert_gain.reshape(1, -1), routes.T, group_weight.reshape(1, -1),
            pair_weight.T, expert_gate[0], expert_up[0], expert_down[0],
            jnp.asarray(rot_t), jnp.asarray(rot_b[:, None, :]),
        )
        return pl.pallas_call(
            place,
            out_shape=(
                jax.ShapeDtypeStruct(mixed.shape, BF16),
                jax.ShapeDtypeStruct(moe.shape, BF16),
            ),
            in_specs=[near, near],
            out_specs=(hbm, hbm),
            scratch_shapes=[DMA((2,))],
        )(*(pltpu.with_memory_space_constraint(v, pltpu.VMEM) for v in (mixed, moe)))

    return jax.shard_map(
        local,
        mesh=mesh,
        in_specs=(
            P(("ep", "tp"), None), P("ep", "tp"), P(), P(None, "tp"), P(None, "tp"),
            P(None, "tp"), P(None, "tp"), P("tp"), P("tp", None), P(("ep", "tp"), None),
            P(), P(("ep", "tp"), None), P(("ep", "tp")), P(("ep", "tp"), None),
            P(("ep", "tp"), None, None), P(("ep", "tp"), None, None),
            P(("ep", "tp"), None, None),
        ),
        out_specs=(P(("ep", "tp"), None), P(("ep", "tp"), None)),
        check_vma=False,
    )
```
